512 devices in a mesh: kv: 32 (over z, core), tp: 16 (over y, x).
Axes of the slice: x: 4, y: 4, z: 16, core: 2. Of those that a mesh axis runs over, the one named last changes fastest.
Arguments:
- tokens: bfloat16 [512, 4096], P(None, 'kv'), may hold values from -40 to 40
- gain_first: float32 [4096], P('kv'), may hold values from 0.1 to 1.9
- gate_first: bfloat16 [4096, 11008], P('kv', 'tp'), may hold values from -0.09375 to 0.09375
- up_first: bfloat16 [4096, 11008], P('kv', 'tp'), may hold values from -0.09375 to 0.09375
- down_first: bfloat16 [11008, 4096], P('tp', 'kv'), may hold values from -0.0546875 to 0.0546875
- gain_mix: float32 [4096], P('kv'), may hold values from 0.1 to 1.9
- w_query: bfloat16 [4096, 2048], P('kv', 'tp'), may hold values from -0.09375 to 0.09375
- w_key: bfloat16 [4096, 2048], P('kv', 'tp'), may hold values from -0.09375 to 0.09375
- w_value: bfloat16 [4096, 2048], P('kv', 'tp'), may hold values from -0.09375 to 0.09375
- w_outgate: bfloat16 [4096, 2048], P('kv', 'tp'), may hold values from -0.09375 to 0.09375
- w_ingate: bfloat16 [4096, 16], P('kv'), may hold values from -0.046875 to 0.046875
- w_forget: bfloat16 [4096, 16], P('kv'), may hold values from -0.09375 to 0.09375
- forget_bias: float32 [16], P('tp'), may hold values from -1 to 4
- memory: float32 [512, 16, 128, 128], P('kv', 'tp'), may hold values from -0.6 to 0.6
- normalizer: float32 [512, 16, 128], P('kv', 'tp'), may hold values from -0.6 to 0.6
- stabilizer: float32 [512, 16], P('kv', 'tp'), may hold values from -3 to 0.5
- w_project: bfloat16 [2048, 4096], P('tp', 'kv'), may hold values from -0.75 to 0.75
- gain_second: float32 [4096], P('kv'), may hold values from 0.3 to 3
- gate_second: bfloat16 [4096, 11008], P('kv', 'tp'), may hold values from -0.09375 to 0.09375
- up_second: bfloat16 [4096, 11008], P('kv', 'tp'), may hold values from -0.09375 to 0.09375
- down_second: bfloat16 [11008, 4096], P('tp', 'kv'), may hold values from -0.0546875 to 0.0546875
Outputs:
- mixed_out: bfloat16 [512, 4096], P(None, 'kv')
- memory_new: float32 [512, 16, 128, 128], P('kv', 'tp')
- normalizer_new: float32 [512, 16, 128], P('kv', 'tp')
- stabilizer_new: float32 [512, 16], P('kv', 'tp')
The draws below stay inside these ranges and needn't reach their ends.
All inputs are finite; a program needn't handle non-finite values.
Results may differ from the reference program's by a relative error of at most 0.04.
Values may be sent and summed in bfloat16 or wider, within the bound.
No kernel may reach another device: no remote copies, remote signals or barrier semaphores. Data moves between devices by JAX's collectives and lax.ppermute only.
A program may use at most 64 MiB of HBM per device.

```python
import math
import jax
import jax.numpy as jnp
from jax import lax

D = 4096
FF = 11008
H = 16
HD = 128
DM = 2048
B = 512
N_KV = 32


def draw_tokens(key, part):
    key_values, key_columns, key_scales = jax.random.split(key, 3)
    col_scales = jnp.exp(jnp.linspace(-1.0, 1.0, D)) * jax.random.uniform(key_columns, (D,), jnp.float32, 0.6, 1.4)
    values = jax.random.normal(key_values, (B, D), jnp.float32)
    row_scales = jnp.exp(jax.random.uniform(key_scales, (B, 1), jnp.float32, -1.1, 1.1))
    return jnp.clip(values * col_scales * row_scales, -40.0, 40.0).astype(jnp.bfloat16)


def block_levels(rng, dims, shards, low, top_value):
    level, own = 1.0, jax.random.fold_in(rng, 6)
    for axis_at, blocks in shards:
        draws = jnp.exp(jax.random.uniform(jax.random.fold_in(own, axis_at), (blocks,), jnp.float32, low / len(shards), top_value / len(shards)))
        level = level * jnp.repeat(draws, dims[axis_at] // blocks).reshape([-1 if axis == axis_at else 1 for axis in range(len(dims))])
    return level


def noise(stream_key, shape, spread, bound, cuts=(), kind=jnp.bfloat16):
    array = jax.random.normal(stream_key, shape, jnp.float32) * spread
    if len(cuts) > 0:
        array = block_levels(stream_key, shape, cuts, -0.22, 0.18) * array
    return jnp.clip(array, min=-bound, max=bound).astype(kind)


def setup_inputs(seed: int = 0) -> dict:
    key_list = jax.random.split(jax.random.key(seed), 22)
    tokens = draw_tokens(jax.random.fold_in(key_list[21], 71), 0)
    gain_first = jnp.clip(1.0 + 0.18 * jax.random.normal(key_list[1], (D,), jnp.float32), 0.1, 1.9)
    gate_first = noise(key_list[2], (D, FF), D ** -0.5, 0.09375, ((0, 32), (1, 16)))
    up_first = noise(key_list[3], (D, FF), D ** -0.5, 0.09375, ((0, 32), (1, 16)))
    down_first = noise(key_list[4], (FF, D), FF ** -0.5, 0.0546875, ((0, 16), (1, 32)))
    gain_mix = jnp.clip(1.0 + 0.18 * jax.random.normal(key_list[5], (D,), jnp.float32), 0.1, 1.9)
    w_query = noise(key_list[6], (D, DM), D ** -0.5, 0.09375, ((0, 32), (1, 16)))
    w_key = noise(key_list[7], (D, DM), D ** -0.5, 0.09375, ((0, 32), (1, 16)))
    w_value = noise(key_list[8], (D, DM), D ** -0.5, 0.09375, ((0, 32), (1, 16)))
    w_outgate = noise(key_list[9], (D, DM), D ** -0.5, 0.09375, ((0, 32), (1, 16)))
    w_ingate = noise(key_list[10], (D, H), (4 * D) ** -0.5, 0.046875, ((0, 32),))
    w_forget = noise(key_list[11], (D, H), D ** -0.5, 0.09375, ((0, 32),))
    forget_bias = jnp.clip(-1.0 + 5.0 * jax.random.uniform(key_list[12], (H,), jnp.float32) ** block_levels(key_list[12], (H,), ((0, 16),), -0.2, 0.2), -1.0, 4.0)
    memory = noise(key_list[13], (B, H, HD, HD), 0.1, 0.6, ((0, 32), (1, 16)), jnp.float32)
    normalizer = noise(key_list[14], (B, H, HD), 0.1, 0.6, ((0, 32), (1, 16)), jnp.float32)
    stabilizer = jnp.clip(-3.0 + 3.5 * jax.random.uniform(key_list[15], (B, H), jnp.float32) ** block_levels(key_list[15], (B, H), ((0, 32), (1, 16)), -0.2, 0.2), -3.0, 0.5)
    w_project = noise(key_list[16], (DM, D), (DM // 32) ** -0.5, 0.75, ((0, 16), (1, 32)))
    gain_second = jnp.clip(jnp.exp(math.log(3.0) - 2.3025851 * jax.random.uniform(key_list[17], (D,), jnp.float32) ** block_levels(key_list[17], (D,), ((0, 32),), -0.2, 0.2)), 0.3, 3.0)
    gate_second = noise(key_list[18], (D, FF), D ** -0.5, 0.09375, ((0, 32), (1, 16)))
    up_second = noise(key_list[19], (D, FF), D ** -0.5, 0.09375, ((0, 32), (1, 16)))
    down_second = noise(key_list[20], (FF, D), FF ** -0.5, 0.0546875, ((0, 16), (1, 32)))
    return dict(tokens=tokens, gain_first=gain_first, gate_first=gate_first, up_first=up_first, down_first=down_first, gain_mix=gain_mix, w_query=w_query, w_key=w_key, w_value=w_value, w_outgate=w_outgate, w_ingate=w_ingate, w_forget=w_forget, forget_bias=forget_bias, memory=memory, normalizer=normalizer, stabilizer=stabilizer, w_project=w_project, gain_second=gain_second, gate_second=gate_second, up_second=up_second, down_second=down_second)


EPSILON = 1e-06

def blockwise(scaled, weight):
    block_rows = weight.shape[0] // N_KV

    def add_block(index, running):
        block_start = index * block_rows
        partial_value = jnp.dot(lax.dynamic_slice_in_dim(scaled, block_start, block_rows, 1), lax.dynamic_slice_in_dim(weight, block_start, block_rows, 0), preferred_element_type=jnp.float32)
        rounded = lax.optimization_barrier(partial_value.astype(jnp.bfloat16))
        return running + rounded.astype(jnp.float32)
    return lax.fori_loop(0, N_KV, add_block, jnp.zeros((scaled.shape[0], weight.shape[1]), jnp.float32))

def row_scaling(widened):
    squared = lax.optimization_barrier(jnp.sum(widened * widened, axis=1, keepdims=True))
    return lax.rsqrt(squared / D + EPSILON)

def half_step(tokens, norm_gain, gate_weight, up_weight, down_weight):
    widened = tokens.astype(jnp.float32)
    row_scale = row_scaling(widened)
    scaled = (widened * norm_gain).astype(jnp.bfloat16)
    gate_values = row_scale * blockwise(scaled, gate_weight)
    up_values = row_scale * blockwise(scaled, up_weight)
    hidden = (jax.nn.silu(gate_values) * up_values).astype(jnp.bfloat16)
    down_values = jnp.dot(hidden, down_weight, preferred_element_type=jnp.float32)
    return (widened + 0.5 * down_values).astype(jnp.bfloat16)

def cell_update(query_bf, key_proj, value_proj, outgate, ingate, forget, memory, normalizer, stabilizer):
    seq_count, heads_here, head_size = normalizer.shape
    query_heads = query_bf.astype(jnp.float32).reshape(seq_count, heads_here, head_size)
    key_heads = key_proj.astype(jnp.float32).reshape(seq_count, heads_here, head_size) * head_size ** (-0.5)
    value_heads = value_proj.astype(jnp.float32).reshape(seq_count, heads_here, head_size)
    log_forget = jax.nn.log_sigmoid(forget)
    ceiling = jnp.maximum(log_forget + stabilizer, ingate)
    fresh_weight = jnp.exp(ingate - ceiling)
    carried = jnp.exp(log_forget + stabilizer - ceiling)
    own_score = lax.optimization_barrier(jnp.sum(query_heads * key_heads, axis=-1)) * fresh_weight
    recall = jnp.einsum('bhde,bhe->bhd', memory, query_heads, precision=lax.Precision.HIGHEST)
    numerator = own_score[..., None] * value_heads + carried[..., None] * recall
    denominator = own_score + carried * lax.optimization_barrier(jnp.sum(normalizer * query_heads, axis=-1))
    readout = numerator / jnp.maximum(jnp.abs(denominator), jnp.exp(-ceiling))[..., None]
    memory_new = carried[..., None, None] * memory + (fresh_weight[..., None] * value_heads)[..., :, None] * key_heads[..., None, :]
    normalizer_new = carried[..., None] * normalizer + fresh_weight[..., None] * key_heads
    gated_out = (jax.nn.sigmoid(outgate.astype(jnp.float32)) * readout.reshape(seq_count, -1)).astype(jnp.bfloat16)
    return (gated_out, memory_new, normalizer_new, ceiling)

def reference(tokens, gain_first, gate_first, up_first, down_first, gain_mix, w_query, w_key, w_value, w_outgate, w_ingate, w_forget, forget_bias, memory, normalizer, stabilizer, w_project, gain_second, gate_second, up_second, down_second):
    after_first = half_step(tokens, gain_first, gate_first, up_first, down_first)
    widened = after_first.astype(jnp.float32)
    row_scale = row_scaling(widened)
    scaled = (widened * gain_mix).astype(jnp.bfloat16)

    def project_heads(weight):
        return (row_scale * blockwise(scaled, weight)).astype(jnp.bfloat16)
    query_bf = project_heads(w_query)
    key_proj = project_heads(w_key)
    value_proj = project_heads(w_value)
    outgate = project_heads(w_outgate)
    ingate = row_scale * blockwise(scaled, w_ingate)
    forget = row_scale * blockwise(scaled, w_forget) + forget_bias
    gated_out, memory_new, normalizer_new, stabilizer_new = cell_update(query_bf, key_proj, value_proj, outgate, ingate, forget, memory, normalizer, stabilizer)
    after_mix = (widened + jnp.dot(gated_out, w_project, preferred_element_type=jnp.float32)).astype(jnp.bfloat16)
    mixed_out = half_step(after_mix, gain_second, gate_second, up_second, down_second)
    return (mixed_out, memory_new, normalizer_new, stabilizer_new)
```

```python
import jax
import jax.numpy as jnp
from jax import lax
from jax.sharding import Mesh
from jax.sharding import PartitionSpec as P

D = 4096
EPSILON = 1e-06
NP = 2
KV = ("zq", "zp", "c")
BF = jnp.bfloat16
F32 = jnp.float32
FFL = 688
HEAD = 640
TAIL = 48


def swap(array):
    return lax.ppermute(array, "zp", [(0, 1), (1, 0)])


def share(array):
    both = jnp.stack([array, swap(array)])
    return lax.all_gather(both, "c")


def copies(array, axis):
    out = jnp.broadcast_to(array, (lax.axis_size(axis), *array.shape))
    return lax.all_to_all(out, axis, split_axis=0, concat_axis=0, tiled=True)


def exchange_sum(parts, axis):
    arrived = lax.all_to_all(parts, axis, split_axis=0, concat_axis=0, tiled=True)
    return jnp.sum(arrived.astype(F32), axis=0)


def pieces(gain):
    hi = gain.astype(BF)
    rest = gain - hi.astype(F32)
    mid = rest.astype(BF)
    low = (rest - mid.astype(F32)).astype(BF)
    return [hi, mid, low]


def gate_up(gate, up):
    zero = jnp.zeros((gate.shape[0], 64 - TAIL), BF)
    return jnp.concatenate(
        [gate[:, :HEAD], up[:, :HEAD], gate[:, HEAD:], zero, up[:, HEAD:], zero], axis=1
    )


def with_squares(product, squares, at):
    hi = squares.astype(BF).astype(F32)
    low = squares - hi
    column = lax.broadcasted_iota(jnp.int32, product.shape, 1)
    return jnp.where(column == at, hi, jnp.where(column == at + 1, low, product))


def row_product(rows, gain, weight, at):
    widened = rows.astype(F32)
    squares = jnp.sum(widened * widened, axis=1, keepdims=True)
    scaled = (widened * gain[None]).astype(BF)
    product = jnp.dot(scaled, weight, preferred_element_type=F32)
    full = with_squares(product, squares, at).astype(BF)
    count = lax.axis_size("zq")
    summed = exchange_sum(full.reshape(count, full.shape[0] // count, full.shape[1]), "zq")
    scale = lax.rsqrt((summed[:, at : at + 1] + summed[:, at + 1 : at + 2]) / D + EPSILON)
    return summed, scale


def tp_sum(partial):
    count = lax.axis_size("tp")
    parts = partial.astype(BF).reshape(count, partial.shape[0] // count, partial.shape[1])
    return exchange_sum(parts, "tp")


def every_row(shard):
    return copies(shard, "tp").reshape(-1, shard.shape[1])


def half_step(rows, residual, gain, weight, down):
    summed, scale = row_product(rows, gain, weight, 1408 - 16)
    gate_head, up_head = summed[:, :HEAD], summed[:, HEAD : 2 * HEAD]
    last = summed[:, 2 * HEAD :]
    gate_tail, up_tail = last[:, :TAIL], last[:, 64 : 64 + TAIL]

    def act(g, u):
        return (jax.nn.silu(scale * g) * (scale * u)).astype(BF)

    hidden = jnp.concatenate([act(gate_head, up_head), act(gate_tail, up_tail)], axis=1)
    hidden_rows = copies(hidden, "zq").reshape(-1, FFL)
    partial = jnp.einsum("rk,bkn->rbn", hidden_rows, down, preferred_element_type=F32)
    update = tp_sum(partial.reshape(partial.shape[0], -1))
    return (residual + 0.5 * update).astype(BF)


def cell_update(query_bf, key_proj, value_proj, outgate, ingate, forget, memory, normalizer, stabilizer):
    seq_count, heads_here, head_size = normalizer.shape
    query_heads = query_bf.astype(F32).reshape(seq_count, heads_here, head_size)
    key_heads = key_proj.astype(F32).reshape(seq_count, heads_here, head_size) * head_size ** (-0.5)
    value_heads = value_proj.astype(F32).reshape(seq_count, heads_here, head_size)
    log_forget = jax.nn.log_sigmoid(forget)
    ceiling = jnp.maximum(log_forget + stabilizer, ingate)
    fresh_weight = jnp.exp(ingate - ceiling)
    carried = jnp.exp(log_forget + stabilizer - ceiling)
    own_score = jnp.sum(query_heads * key_heads, axis=-1) * fresh_weight
    recall = jnp.einsum("bhde,bhe->bhd", memory, query_heads, precision=lax.Precision.HIGHEST)
    numerator = own_score[..., None] * value_heads + carried[..., None] * recall
    denominator = own_score + carried * jnp.sum(normalizer * query_heads, axis=-1)
    readout = numerator / jnp.maximum(jnp.abs(denominator), jnp.exp(-ceiling))[..., None]
    memory_new = (
        carried[..., None, None] * memory
        + (fresh_weight[..., None] * value_heads)[..., :, None] * key_heads[..., None, :]
    )
    normalizer_new = carried[..., None] * normalizer + fresh_weight[..., None] * key_heads
    gated_out = (
        jax.nn.sigmoid(outgate.astype(F32)) * readout.reshape(seq_count, -1)
    ).astype(BF)
    return (gated_out, memory_new, normalizer_new, ceiling)


def on_device(
    tokens,
    gain_first,
    gate_first,
    up_first,
    down_first,
    gain_mix,
    w_query,
    w_key,
    w_value,
    w_outgate,
    w_ingate,
    w_forget,
    forget_bias,
    memory,
    normalizer,
    stabilizer,
    w_project,
    gain_second,
    gate_second,
    up_second,
    down_second,
):
    pair = lax.axis_index("zp")
    core = lax.axis_index("c")
    nq = lax.axis_size("zq")
    nt = lax.axis_size("tp")
    seqs = tokens.shape[0] // (nq * NP * 2)
    width = tokens.shape[1]
    row_count = nq * seqs
    shard_rows = row_count // nt

    grouped = tokens.reshape(nq, NP, 2, seqs, width).transpose(1, 2, 0, 3, 4)
    grouped = grouped.reshape(NP, 2, row_count, width)
    gains = jnp.stack(pieces(gain_first) + pieces(gain_mix) + pieces(gain_second))
    gains = jnp.concatenate([gains, jnp.zeros((16 - gains.shape[0], width), BF)])
    kept = lax.dynamic_index_in_dim(grouped, pair, 0, keepdims=False)
    sent = lax.dynamic_index_in_dim(grouped, 1 - pair, 0, keepdims=False)

    def packed(rows):
        return jnp.concatenate([rows.reshape(2 * row_count, width), gains])

    came = swap(packed(sent))
    here = lax.all_gather(jnp.stack([packed(kept), came]), "c")
    row_part = here[:, :, : 2 * row_count].reshape(2, NP, 2, row_count, width)
    mine = lax.dynamic_index_in_dim(row_part, core, 2, keepdims=False)
    rows = mine.transpose(2, 0, 1, 3).reshape(row_count, 2 * NP * width)
    gain_part = here[:, :, 2 * row_count :].astype(F32)
    gain_all = [
        ((gain_part[:, :, 3 * i] + gain_part[:, :, 3 * i + 1]) + gain_part[:, :, 3 * i + 2]).reshape(-1)
        for i in range(3)
    ]

    first_in = share(gate_up(gate_first, up_first)).reshape(2 * NP * width, -1)
    gates = jnp.concatenate(
        [w_ingate, w_forget, jnp.zeros((width, 128 - 2 * w_ingate.shape[1]), BF)], axis=1
    )
    later = share(
        jnp.concatenate(
            [w_query, w_key, w_value, w_outgate, gates, gate_up(gate_second, up_second)], axis=1
        )
    ).reshape(2 * NP * width, -1)
    outs = share(jnp.concatenate([down_first, w_project, down_second]))
    outs = outs.reshape(2 * NP, -1, width)
    mix_in, second_in = later[:, :640], later[:, 640:]
    down_one = outs[:, :FFL]
    project = outs[:, FFL : FFL + 128]
    down_two = outs[:, FFL + 128 :]

    shard_at = lax.axis_index("tp") * shard_rows
    residual = lax.dynamic_slice_in_dim(rows, shard_at, shard_rows, 0).astype(F32)
    after_first = half_step(rows, residual, gain_all[0], first_in, down_one)

    heads = w_ingate.shape[1]
    summed, scale = row_product(every_row(after_first), gain_all[1], mix_in, 512 + 2 * heads)
    query_bf, key_proj, value_proj, outgate = (
        (scale * summed[:, 128 * i : 128 * (i + 1)]).astype(BF) for i in range(4)
    )
    at = lax.axis_index("tp")
    ingate = scale * lax.dynamic_slice_in_dim(summed[:, 512 : 512 + heads], at, 1, 1)
    forget = scale * lax.dynamic_slice_in_dim(summed[:, 512 + heads : 512 + 2 * heads], at, 1, 1)
    gated_out, memory_new, normalizer_new, stabilizer_new = cell_update(
        query_bf, key_proj, value_proj, outgate, ingate, forget + forget_bias, memory, normalizer, stabilizer
    )
    gated_rows = copies(gated_out, "zq").reshape(row_count, -1)
    mixed = jnp.einsum("rk,bkn->rbn", gated_rows, project, preferred_element_type=F32)
    after_mix = (
        after_first.astype(F32) + tp_sum(mixed.reshape(row_count, -1))
    ).astype(BF)

    last = half_step(
        every_row(after_mix), after_mix.astype(F32), gain_all[2], second_in, down_two
    )
    columns = last.reshape(shard_rows, 2, NP, width).transpose(2, 1, 0, 3)
    columns = jnp.where(pair == 0, columns, columns[::-1])
    outgoing = jnp.broadcast_to(
        columns[:, :, None], (NP, 2, nt, shard_rows, width)
    ).reshape(NP * 2 * nt, shard_rows, width)
    came = lax.all_to_all(outgoing, ("zp", "c", "tp"), 0, 0, tiled=True)
    came = came.reshape(NP, 2, nq, seqs, width).transpose(2, 0, 1, 3, 4)
    return (came.reshape(-1, width), memory_new, normalizer_new, stabilizer_new)


def solution(mesh):
    kv, tp = mesh.shape["kv"], mesh.shape["tp"]
    finer = Mesh(mesh.devices.reshape(kv // (2 * NP), NP, 2, tp), ("zq", "zp", "c", "tp"))
    return jax.shard_map(
        on_device,
        mesh=finer,
        in_specs=(
            P(None, KV),
            P(KV),
            P(KV, "tp"),
            P(KV, "tp"),
            P("tp", KV),
            P(KV),
            P(KV, "tp"),
            P(KV, "tp"),
            P(KV, "tp"),
            P(KV, "tp"),
            P(KV, None),
            P(KV, None),
            P("tp"),
            P(KV, "tp", None, None),
            P(KV, "tp", None),
            P(KV, "tp"),
            P("tp", KV),
            P(KV),
            P(KV, "tp"),
            P(KV, "tp"),
            P("tp", KV),
        ),
        out_specs=(P(None, KV), P(KV, "tp", None, None), P(KV, "tp", None), P(KV, "tp")),
        check_vma=False,
    )
```

```python
import jax
import jax.numpy as jnp
from jax import lax
from jax.experimental import pallas as pl
from jax.experimental.pallas import tpu as pltpu
from jax.sharding import Mesh
from jax.sharding import PartitionSpec as P


D = 4096
EPSILON = 1e-06
NP = 2
KV = ("zq", "zp", "c")
BF = jnp.bfloat16
F32 = jnp.float32
FFL = 688
HEAD = 640
TAIL = 48
WIDE = 1408
MIX = 640
NT_DIMS = (((1,), (1,)), ((), ()))


def swap(array):
    return lax.ppermute(array, "zp", [(0, 1), (1, 0)])


def both_cores(array):
    return lax.all_gather(array, "c")


def exchange(parts, axis):
    return lax.all_to_all(parts, axis, split_axis=0, concat_axis=0, tiled=True)


def pieces(gain):
    hi = gain.astype(BF)
    rest = gain - hi.astype(F32)
    mid = rest.astype(BF)
    low = (rest - mid.astype(F32)).astype(BF)
    return [hi, mid, low]


def gate_up(gate, up):
    return [
        (gate, 0, HEAD),
        (up, 0, HEAD),
        (gate, HEAD, TAIL),
        (gate, 0, 64 - TAIL),
        (up, HEAD, TAIL),
        (up, 0, 64 - TAIL),
    ]


def scaled_rows(x_ref, gain_ref):
    groups, rows, width = x_ref.shape
    x = x_ref[...].astype(F32).reshape(groups * rows, width)
    squares = jnp.sum(x * x, axis=1, keepdims=True)
    return (x * gain_ref[...]).astype(BF), squares


def put_squares(block, squares, at):
    hi = squares.astype(BF).astype(F32)
    low = squares - hi
    column = lax.broadcasted_iota(jnp.int32, block.shape, 1)
    return jnp.where(column == at, hi, jnp.where(column == at + 1, low, block))


def dot(a, b, dims=(((1,), (0,)), ((), ()))):
    return lax.dot_general(a, b, dims, preferred_element_type=F32)


def wide_kernel(x_ref, gain_ref, own_ref, other_ref, out_ref):
    scaled, squares = scaled_rows(x_ref, gain_ref)
    total = None
    for core in range(2):
        weight = jnp.concatenate([own_ref[core, :WIDE], other_ref[core, :WIDE]], axis=1)
        part = dot(scaled[:, 256 * core : 256 * (core + 1)], weight, NT_DIMS)
        total = part if total is None else total + part
    out_ref[:, : WIDE - 128] = total[:, : WIDE - 128].astype(BF)
    out_ref[:, WIDE - 128 :] = put_squares(total[:, WIDE - 128 :], squares, 112).astype(BF)


def prep_kernel(pair_ref, tokens_ref, first_ref, mix_ref, second_ref, kept_ref, sent_ref):
    gains = []
    for ref in (first_ref, mix_ref, second_ref):
        gains += pieces(ref[...])
    for ref, which in ((kept_ref, pair_ref[0]), (sent_ref, 1 - pair_ref[0])):
        for core in range(2):
            for group in range(8):
                at = 128 * core + 16 * group
                ref[at : at + 16] = tokens_ref[group, which, core]
        rows = [g.astype(F32) for g in gains] + [jnp.zeros((7, 128), F32)]
        ref[256:] = jnp.concatenate(rows, axis=0).astype(BF)


def pack_kernel(plan):
    def kernel(*refs):
        sources, out, sems = refs[:-2], refs[-2], refs[-1]
        started, at = [], 0
        for i, (source, start, count) in enumerate(plan):
            copy = pltpu.make_async_copy(
                sources[source].at[pl.ds(start, count)], out.at[pl.ds(at, count)], sems.at[i]
            )
            copy.start()
            started.append(copy)
            at += count
        for copy in started:
            copy.wait()

    return kernel


def pack(plan, *arrays):
    anywhere = pl.BlockSpec(memory_space=pl.ANY)
    return pl.pallas_call(
        pack_kernel(plan),
        in_specs=[pl.BlockSpec(memory_space=pltpu.HBM)] * len(arrays),
        out_specs=anywhere,
        out_shape=jax.ShapeDtypeStruct((sum(count for _, _, count in plan), 128), BF),
        scratch_shapes=[pltpu.SemaphoreType.DMA((len(plan),))],
        compiler_params=pltpu.CompilerParams(vmem_limit_bytes=2**20),
    )(*arrays)


def first_kernel(core_ref, kept_ref, came_ref, own_ref, other_ref, out_ref, rows_ref, gains_ref):
    start = pl.multiple_of(128 * core_ref[0], 128)
    total, squares = None, None
    for core in range(2):
        x, gain = [], []
        for chip, here_ref in enumerate((kept_ref, came_ref)):
            at = 128 * (2 * core + chip)
            block = here_ref[core, pl.ds(start, 128)]
            rows_ref[:, :, at : at + 128] = block.reshape(16, 8, 128)
            x.append(block.astype(F32))
            parts = here_ref[core, 256:].astype(F32)
            for i in range(3):
                whole = (parts[3 * i : 3 * i + 1] + parts[3 * i + 1 : 3 * i + 2]) + parts[
                    3 * i + 2 : 3 * i + 3
                ]
                gains_ref[i, :, at : at + 128] = whole
                if i == 0:
                    gain.append(whole)
        x, gain = jnp.concatenate(x, axis=1), jnp.concatenate(gain, axis=1)
        square = jnp.sum(x * x, axis=1, keepdims=True)
        squares = square if squares is None else squares + square
        weight = jnp.concatenate([own_ref[core, :WIDE], other_ref[core, :WIDE]], axis=1)
        part = dot((x * gain).astype(BF), weight, NT_DIMS)
        total = part if total is None else total + part
    out_ref[:, : WIDE - 128] = total[:, : WIDE - 128].astype(BF)
    out_ref[:, WIDE - 128 :] = put_squares(total[:, WIDE - 128 :], squares, 112).astype(BF)


def mix_kernel(x_ref, gain_ref, own_ref, other_ref, out_ref):
    scaled, squares = scaled_rows(x_ref, gain_ref)
    for pair in range(2):
        total = None
        for core in range(2):
            columns = [
                jnp.concatenate(
                    [own_ref[core, 128 * m : 128 * (m + 1)], other_ref[core, 128 * m : 128 * (m + 1)]],
                    axis=0,
                )
                for m in (2 * pair, 2 * pair + 1)
            ]
            part = dot(scaled[:, 256 * core : 256 * (core + 1)], jnp.concatenate(columns, axis=1))
            total = part if total is None else total + part
        out_ref[:, 256 * pair : 256 * (pair + 1)] = total.astype(BF)
    total = None
    for core in range(2):
        weight = jnp.concatenate([own_ref[core, 512:544], other_ref[core, 512:544]], axis=1)
        weight = jnp.concatenate([weight, jnp.zeros((128 - weight.shape[0], 256), BF)], axis=0)
        part = dot(scaled[:, 256 * core : 256 * (core + 1)], weight, NT_DIMS)
        total = part if total is None else total + part
    out_ref[:, 512:] = put_squares(total, squares, 112).astype(BF)


def act_kernel(x_ref, out_ref):
    total = x_ref[0].astype(F32)
    for i in range(1, x_ref.shape[0]):
        total = total + x_ref[i].astype(F32)
    last = total[:, WIDE - 128 :]
    scale = lax.rsqrt((last[:, 112:113] + last[:, 113:114]) / D + EPSILON)

    def act(gate, up):
        gate, up = scale * gate, scale * up
        return (gate * jax.nn.sigmoid(gate) * up).astype(BF)

    head = act(total[:, :HEAD], total[:, HEAD : 2 * HEAD])
    tail = act(last, pltpu.roll(last, 64, 1))[:, :TAIL]
    for i in range(out_ref.shape[0]):
        out_ref[i, :, :HEAD] = head
        out_ref[i, :, HEAD:] = tail


def out_kernel(spans):
    def kernel(x_ref, *refs):
        out_ref = refs[-1]
        groups, rows, width = x_ref.shape
        x = x_ref[...].reshape(groups * rows, width)
        for core in range(2):
            columns = []
            for chip in range(2):
                blocks = [
                    refs[2 * source + chip][core, start : start + count]
                    for source, start, count in spans
                ]
                columns.append(blocks[0] if len(blocks) == 1 else jnp.concatenate(blocks, axis=0))
            part = dot(x, jnp.concatenate(columns, axis=1)).astype(BF)
            out_ref[:, 256 * core : 256 * (core + 1)] = part

    return kernel


def residual_kernel(factor):
    def kernel(at_ref, sum_ref, old_ref, new_ref, copies_ref):
        total = sum_ref[0].astype(F32)
        for i in range(1, sum_ref.shape[0]):
            total = total + sum_ref[i].astype(F32)
        new = (old_ref[at_ref[0]].astype(F32) + factor * total).astype(BF)
        new_ref[0] = new
        for i in range(copies_ref.shape[0]):
            copies_ref[i] = new

    return kernel


def last_kernel(at_ref, sum_ref, old_ref, out_ref):
    total = sum_ref[0].astype(F32)
    for i in range(1, sum_ref.shape[0]):
        total = total + sum_ref[i].astype(F32)
    new = (old_ref[0].astype(F32) + 0.5 * total).astype(BF)
    first = at_ref[0] == 0
    for core in range(2):
        own = new[:, 256 * core : 256 * core + 128]
        other = new[:, 256 * core + 128 : 256 * (core + 1)]
        blocks = (jnp.where(first, own, other), jnp.where(first, other, own))
        for pair in range(2):
            for i in range(16):
                out_ref[(2 * pair + core) * 16 + i] = blocks[pair]


def call(kernel, out_shapes, scalars=0):
    smem = pl.BlockSpec(memory_space=pltpu.SMEM)
    vmem = pl.BlockSpec(memory_space=pltpu.VMEM)

    def run(*args):
        return pl.pallas_call(
            kernel,
            in_specs=[smem] * scalars + [vmem] * (len(args) - scalars),
            out_specs=jax.tree.map(lambda s: vmem, out_shapes),
            out_shape=out_shapes,
            compiler_params=pltpu.CompilerParams(vmem_limit_bytes=12 * 2**20),
        )(*args)

    return run


def half_step(wide, down):
    came = exchange(wide.reshape(8, 16, WIDE), "zq")
    hidden = call(act_kernel, jax.ShapeDtypeStruct((8, 16, FFL), BF))(came)
    hidden = exchange(hidden, "zq")
    spans, weights = down
    part = call(out_kernel(spans), jax.ShapeDtypeStruct((128, 512), BF))(hidden, *weights)
    return exchange(part.reshape(16, 8, 512), "tp")


def cell_update(query_bf, key_proj, value_proj, outgate, ingate, forget, memory, normalizer, stabilizer):
    seq_count, heads_here, head_size = normalizer.shape
    query_heads = query_bf.astype(F32).reshape(seq_count, heads_here, head_size)
    key_heads = key_proj.astype(F32).reshape(seq_count, heads_here, head_size) * head_size ** (-0.5)
    value_heads = value_proj.astype(F32).reshape(seq_count, heads_here, head_size)
    log_forget = jax.nn.log_sigmoid(forget)
    ceiling = jnp.maximum(log_forget + stabilizer, ingate)
    fresh_weight = jnp.exp(ingate - ceiling)
    carried = jnp.exp(log_forget + stabilizer - ceiling)
    own_score = jnp.sum(query_heads * key_heads, axis=-1) * fresh_weight
    recall = jnp.einsum("bhde,bhe->bhd", memory, query_heads, precision=lax.Precision.HIGHEST)
    numerator = own_score[..., None] * value_heads + carried[..., None] * recall
    denominator = own_score + carried * jnp.sum(normalizer * query_heads, axis=-1)
    readout = numerator / jnp.maximum(jnp.abs(denominator), jnp.exp(-ceiling))[..., None]
    memory_new = (
        carried[..., None, None] * memory
        + (fresh_weight[..., None] * value_heads)[..., :, None] * key_heads[..., None, :]
    )
    normalizer_new = carried[..., None] * normalizer + fresh_weight[..., None] * key_heads
    gated_out = (
        jax.nn.sigmoid(outgate.astype(F32)) * readout.reshape(seq_count, -1)
    ).astype(BF)
    return (gated_out, memory_new, normalizer_new, ceiling)


def on_device(
    tokens,
    gain_first,
    gate_first,
    up_first,
    down_first,
    gain_mix,
    w_query,
    w_key,
    w_value,
    w_outgate,
    w_ingate,
    w_forget,
    forget_bias,
    memory,
    normalizer,
    stabilizer,
    w_project,
    gain_second,
    gate_second,
    up_second,
    down_second,
):
    pair = lax.axis_index("zp")
    core = lax.axis_index("c")
    at = lax.axis_index("tp")

    pair_at = jnp.reshape(pair, (1,)).astype(jnp.int32)
    core_at = jnp.reshape(core, (1,)).astype(jnp.int32)
    shard_at = jnp.reshape(at, (1,)).astype(jnp.int32)
    zero = jnp.zeros((1,), jnp.int32)
    wide_shape = jax.ShapeDtypeStruct((128, WIDE), BF)

    first = pack(gate_up(0, 1), gate_first.T, up_first.T)
    first_came = swap(first)
    packed = jax.ShapeDtypeStruct((272, 128), BF)
    kept, sent = call(prep_kernel, (packed, packed), 1)(
        pair_at,
        tokens.reshape(8, NP, 2, 16, 128),
        gain_first.reshape(1, 128),
        gain_mix.reshape(1, 128),
        gain_second.reshape(1, 128),
    )
    came = swap(sent)
    heads = w_ingate.shape[1]
    middle = pack(
        [(i, 0, 128) for i in range(4)]
        + [(4, 0, heads), (5, 0, heads), (6, 0, FFL), (7, 0, 128), (8, FFL - 64, 64)],
        w_query,
        w_key,
        w_value,
        w_outgate,
        w_ingate.T,
        w_forget.T,
        down_first,
        w_project,
        down_second,
    )
    middle_came = swap(middle)
    last = pack(gate_up(0, 1) + [(2, 0, FFL - 64)], gate_second.T, up_second.T, down_second)
    last_came = swap(last)

    kept, came = both_cores(kept), both_cores(came)
    first_own, first_other = both_cores(first), both_cores(first_came)
    middle_own = both_cores(middle)
    middle_other = both_cores(middle_came)
    last_own = both_cores(last)
    last_other = both_cores(last_came)

    shard = jax.ShapeDtypeStruct((1, 8, 512), BF)
    copied = jax.ShapeDtypeStruct((16, 8, 512), BF)
    wide, rows, gains = call(
        first_kernel, (wide_shape, copied, jax.ShapeDtypeStruct((3, 1, 512), F32)), 1
    )(core_at, kept, came, first_own, first_other)
    came = half_step(wide, (((0, 544, FFL),), (middle_own, middle_other)))
    after_first, copies = call(residual_kernel(0.5), (shard, copied), 1)(shard_at, came, rows)
    copies = exchange(copies, "tp")

    mixed = call(mix_kernel, jax.ShapeDtypeStruct((128, MIX), BF))(
        copies, gains[1], middle_own, middle_other
    )
    summed = exchange(mixed.reshape(8, 16, MIX), "zq")
    summed = jnp.sum(summed.astype(F32), axis=0)
    scale = lax.rsqrt((summed[:, 624:625] + summed[:, 625:626]) / D + EPSILON)
    query_bf, key_proj, value_proj, outgate = (
        (scale * summed[:, 128 * i : 128 * (i + 1)]).astype(BF) for i in range(4)
    )
    ingate = scale * lax.dynamic_slice_in_dim(summed[:, 512 : 512 + heads], at, 1, 1)
    forget = scale * lax.dynamic_slice_in_dim(summed[:, 512 + heads : 512 + 2 * heads], at, 1, 1)
    gated_out, memory_new, normalizer_new, stabilizer_new = cell_update(
        query_bf, key_proj, value_proj, outgate, ingate, forget + forget_bias, memory, normalizer, stabilizer
    )
    gated = exchange(jnp.broadcast_to(gated_out, (8, *gated_out.shape)), "zq")
    part = call(out_kernel(((0, 1232, 128),)), jax.ShapeDtypeStruct((128, 512), BF))(
        gated, middle_own, middle_other
    )
    came = exchange(part.reshape(16, 8, 512), "tp")
    after_mix, copies = call(residual_kernel(1.0), (shard, copied), 1)(zero, came, after_first)
    copies = exchange(copies, "tp")

    wide = call(wide_kernel, wide_shape)(copies, gains[2], last_own, last_other)
    came = half_step(
        wide,
        (
            ((0, WIDE, FFL - 64), (1, 1360, 64)),
            (last_own, last_other, middle_own, middle_other),
        ),
    )
    outgoing = call(last_kernel, jax.ShapeDtypeStruct((64, 8, 128), BF), 1)(
        pair_at, came, after_mix
    )
    came = exchange(outgoing, ("zp", "c", "tp"))
    came = came.reshape(NP, 2, 8, 16, 128).transpose(2, 0, 1, 3, 4)
    return (came.reshape(-1, 128), memory_new, normalizer_new, stabilizer_new)


def solution(mesh):
    kv, tp = mesh.shape["kv"], mesh.shape["tp"]
    finer = Mesh(mesh.devices.reshape(kv // (2 * NP), NP, 2, tp), ("zq", "zp", "c", "tp"))
    return jax.shard_map(
        on_device,
        mesh=finer,
        in_specs=(
            P(None, KV),
            P(KV),
            P(KV, "tp"),
            P(KV, "tp"),
            P("tp", KV),
            P(KV),
            P(KV, "tp"),
            P(KV, "tp"),
            P(KV, "tp"),
            P(KV, "tp"),
            P(KV, None),
            P(KV, None),
            P("tp"),
            P(KV, "tp", None, None),
            P(KV, "tp", None),
            P(KV, "tp"),
            P("tp", KV),
            P(KV),
            P(KV, "tp"),
            P(KV, "tp"),
            P("tp", KV),
        ),
        out_specs=(P(None, KV), P(KV, "tp", None, None), P(KV, "tp", None), P(KV, "tp")),
        check_vma=False,
    )
```

```python
import jax
import jax.numpy as jnp
from jax import lax
from jax.experimental import pallas as pl
from jax.experimental.pallas import tpu as pltpu
from jax.sharding import Mesh
from jax.sharding import PartitionSpec as P


D = 4096
EPSILON = 1e-06
NP = 2
KV = ("zq", "zp", "c")
BF = jnp.bfloat16
F32 = jnp.float32
FFL = 688
HEAD = 640
TAIL = 48
WIDE = 1408
MIX = 640
HERE = 272
NT_DIMS = (((1,), (1,)), ((), ()))


def swap(array):
    return lax.ppermute(array, "zp", [(0, 1), (1, 0)])


def both_cores(array):
    return lax.all_gather(array, "c")


def exchange(parts, axis):
    return lax.all_to_all(parts, axis, split_axis=0, concat_axis=0, tiled=True)


def pieces(gain):
    hi = gain.astype(BF)
    rest = gain - hi.astype(F32)
    mid = rest.astype(BF)
    low = (rest - mid.astype(F32)).astype(BF)
    return [hi, mid, low]


def gate_up(gate, up):
    return [
        (gate, 0, HEAD),
        (up, 0, HEAD),
        (gate, HEAD, TAIL),
        (gate, 0, 64 - TAIL),
        (up, HEAD, TAIL),
        (up, 0, 64 - TAIL),
    ]


def scaled_rows(x_ref, gain_ref):
    groups, rows, width = x_ref.shape
    x = x_ref[...].astype(F32).reshape(groups * rows, width)
    squares = jnp.sum(x * x, axis=1, keepdims=True)
    return (x * gain_ref[...]).astype(BF), squares


def put_squares(block, squares, at):
    hi = squares.astype(BF).astype(F32)
    low = squares - hi
    column = lax.broadcasted_iota(jnp.int32, block.shape, 1)
    return jnp.where(column == at, hi, jnp.where(column == at + 1, low, block))


def dot(a, b, dims=(((1,), (0,)), ((), ()))):
    return lax.dot_general(a, b, dims, preferred_element_type=F32)


def wide_kernel(x_ref, gain_ref, own_ref, other_ref, out_ref):
    scaled, squares = scaled_rows(x_ref, gain_ref)
    total = None
    for core in range(2):
        weight = jnp.concatenate([own_ref[core, :WIDE], other_ref[core, :WIDE]], axis=1)
        part = dot(scaled[:, 256 * core : 256 * (core + 1)], weight, NT_DIMS)
        total = part if total is None else total + part
    out_ref[:, : WIDE - 128] = total[:, : WIDE - 128].astype(BF)
    out_ref[:, WIDE - 128 :] = put_squares(total[:, WIDE - 128 :], squares, 112).astype(BF)


def prep_kernel(pair_ref, tokens_ref, first_ref, mix_ref, second_ref, gate_ref, up_ref, *refs):
    kept_ref, sent_ref, sems = refs
    copies = []
    for ref in (kept_ref, sent_ref):
        at = HERE
        for source, start, count in gate_up(gate_ref, up_ref):
            copy = pltpu.make_async_copy(
                source.at[pl.ds(start, count)], ref.at[pl.ds(at, count)], sems.at[len(copies)]
            )
            copy.start()
            copies.append(copy)
            at += count
    gains = []
    for ref in (first_ref, mix_ref, second_ref):
        gains += pieces(ref[...])
    rows = [g.astype(F32) for g in gains] + [jnp.zeros((7, 128), F32)]
    rows = jnp.concatenate(rows, axis=0).astype(BF)
    for ref, which in ((kept_ref, pair_ref[0]), (sent_ref, 1 - pair_ref[0])):
        for core in range(2):
            for group in range(8):
                at = 128 * core + 16 * group
                ref[at : at + 16] = tokens_ref[group, which, core]
        ref[256:HERE] = rows
    for copy in copies:
        copy.wait()


def pack_kernel(plan):
    def kernel(*refs):
        sources, out, sems = refs[:-2], refs[-2], refs[-1]
        started, at = [], 0
        for i, (source, start, count) in enumerate(plan):
            copy = pltpu.make_async_copy(
                sources[source].at[pl.ds(start, count)], out.at[pl.ds(at, count)], sems.at[i]
            )
            copy.start()
            started.append(copy)
            at += count
        for copy in started:
            copy.wait()

    return kernel


def pack(plan, *arrays):
    anywhere = pl.BlockSpec(memory_space=pl.ANY)
    return pl.pallas_call(
        pack_kernel(plan),
        in_specs=[pl.BlockSpec(memory_space=pltpu.HBM)] * len(arrays),
        out_specs=anywhere,
        out_shape=jax.ShapeDtypeStruct((sum(count for _, _, count in plan), 128), BF),
        scratch_shapes=[pltpu.SemaphoreType.DMA((len(plan),))],
        compiler_params=pltpu.CompilerParams(vmem_limit_bytes=2**20),
    )(*arrays)


def first_kernel(core_ref, own_ref, other_ref, out_ref, rows_ref, gains_ref):
    start = pl.multiple_of(128 * core_ref[0], 128)
    total, squares = None, None
    for core in range(2):
        x, gain = [], []
        for chip, here_ref in enumerate((own_ref, other_ref)):
            at = 128 * (2 * core + chip)
            block = here_ref[core, pl.ds(start, 128)]
            rows_ref[:, :, at : at + 128] = block.reshape(16, 8, 128)
            x.append(block.astype(F32))
            parts = here_ref[core, 256:HERE].astype(F32)
            for i in range(3):
                whole = (parts[3 * i : 3 * i + 1] + parts[3 * i + 1 : 3 * i + 2]) + parts[
                    3 * i + 2 : 3 * i + 3
                ]
                gains_ref[i, :, at : at + 128] = whole
                if i == 0:
                    gain.append(whole)
        x, gain = jnp.concatenate(x, axis=1), jnp.concatenate(gain, axis=1)
        square = jnp.sum(x * x, axis=1, keepdims=True)
        squares = square if squares is None else squares + square
        weight = jnp.concatenate([own_ref[core, HERE:], other_ref[core, HERE:]], axis=1)
        part = dot((x * gain).astype(BF), weight, NT_DIMS)
        total = part if total is None else total + part
    out_ref[:, : WIDE - 128] = total[:, : WIDE - 128].astype(BF)
    out_ref[:, WIDE - 128 :] = put_squares(total[:, WIDE - 128 :], squares, 112).astype(BF)


def mix_kernel(x_ref, gain_ref, own_ref, other_ref, out_ref):
    scaled, squares = scaled_rows(x_ref, gain_ref)
    for pair in range(2):
        total = None
        for core in range(2):
            columns = [
                jnp.concatenate(
                    [own_ref[core, 128 * m : 128 * (m + 1)], other_ref[core, 128 * m : 128 * (m + 1)]],
                    axis=0,
                )
                for m in (2 * pair, 2 * pair + 1)
            ]
            part = dot(scaled[:, 256 * core : 256 * (core + 1)], jnp.concatenate(columns, axis=1))
            total = part if total is None else total + part
        out_ref[:, 256 * pair : 256 * (pair + 1)] = total.astype(BF)
    total = None
    for core in range(2):
        weight = jnp.concatenate([own_ref[core, 512:544], other_ref[core, 512:544]], axis=1)
        weight = jnp.concatenate([weight, jnp.zeros((128 - weight.shape[0], 256), BF)], axis=0)
        part = dot(scaled[:, 256 * core : 256 * (core + 1)], weight, NT_DIMS)
        total = part if total is None else total + part
    out_ref[:, 512:] = put_squares(total, squares, 112).astype(BF)


def act_kernel(x_ref, out_ref):
    total = x_ref[0].astype(F32)
    for i in range(1, x_ref.shape[0]):
        total = total + x_ref[i].astype(F32)
    last = total[:, WIDE - 128 :]
    scale = lax.rsqrt((last[:, 112:113] + last[:, 113:114]) / D + EPSILON)

    def act(gate, up):
        gate, up = scale * gate, scale * up
        return (gate * jax.nn.sigmoid(gate) * up).astype(BF)

    head = act(total[:, :HEAD], total[:, HEAD : 2 * HEAD])
    tail = act(last, pltpu.roll(last, 64, 1))[:, :TAIL]
    for i in range(out_ref.shape[0]):
        out_ref[i, :, :HEAD] = head
        out_ref[i, :, HEAD:] = tail


def out_kernel(spans):
    def kernel(x_ref, *refs):
        out_ref = refs[-1]
        groups, rows, width = x_ref.shape
        x = x_ref[...].reshape(groups * rows, width)
        for core in range(2):
            columns = []
            for chip in range(2):
                blocks = [
                    refs[2 * source + chip][core, start : start + count]
                    for source, start, count in spans
                ]
                columns.append(blocks[0] if len(blocks) == 1 else jnp.concatenate(blocks, axis=0))
            part = dot(x, jnp.concatenate(columns, axis=1)).astype(BF)
            out_ref[:, 256 * core : 256 * (core + 1)] = part

    return kernel


def residual_kernel(factor):
    def kernel(at_ref, sum_ref, old_ref, new_ref, copies_ref):
        total = sum_ref[0].astype(F32)
        for i in range(1, sum_ref.shape[0]):
            total = total + sum_ref[i].astype(F32)
        new = (old_ref[at_ref[0]].astype(F32) + factor * total).astype(BF)
        new_ref[0] = new
        for i in range(copies_ref.shape[0]):
            copies_ref[i] = new

    return kernel


def last_kernel(at_ref, sum_ref, old_ref, out_ref):
    total = sum_ref[0].astype(F32)
    for i in range(1, sum_ref.shape[0]):
        total = total + sum_ref[i].astype(F32)
    new = (old_ref[0].astype(F32) + 0.5 * total).astype(BF)
    first = at_ref[0] == 0
    for core in range(2):
        own = new[:, 256 * core : 256 * core + 128]
        other = new[:, 256 * core + 128 : 256 * (core + 1)]
        blocks = (jnp.where(first, own, other), jnp.where(first, other, own))
        for pair in range(2):
            for i in range(16):
                out_ref[(2 * pair + core) * 16 + i] = blocks[pair]


def call(kernel, out_shapes, scalars=0):
    smem = pl.BlockSpec(memory_space=pltpu.SMEM)
    vmem = pl.BlockSpec(memory_space=pltpu.VMEM)

    def run(*args):
        return pl.pallas_call(
            kernel,
            in_specs=[smem] * scalars + [vmem] * (len(args) - scalars),
            out_specs=jax.tree.map(lambda s: vmem, out_shapes),
            out_shape=out_shapes,
            compiler_params=pltpu.CompilerParams(vmem_limit_bytes=12 * 2**20),
        )(*args)

    return run


def half_step(wide, down):
    came = exchange(wide.reshape(8, 16, WIDE), "zq")
    hidden = call(act_kernel, jax.ShapeDtypeStruct((8, 16, FFL), BF))(came)
    hidden = exchange(hidden, "zq")
    spans, weights = down
    part = call(out_kernel(spans), jax.ShapeDtypeStruct((128, 512), BF))(hidden, *weights)
    return exchange(part.reshape(16, 8, 512), "tp")


def cell_kernel(at_ref, bias_ref, x_ref, memory_ref, normalizer_ref, stabilizer_ref, *out_refs):
    copies_ref, carried_ref, value_ref, key_ref, normalizer_out, stabilizer_out = out_refs
    total = x_ref[0].astype(F32)
    for i in range(1, x_ref.shape[0]):
        total = total + x_ref[i].astype(F32)
    gates = total[:, 512:]
    scale = lax.rsqrt((gates[:, 112:113] + gates[:, 113:114]) / D + EPSILON)
    query, key, value, outgate = (
        (scale * total[:, 128 * i : 128 * (i + 1)]).astype(BF).astype(F32) for i in range(4)
    )
    key = key * 128 ** (-0.5)
    column = lax.broadcasted_iota(jnp.int32, gates.shape, 1)

    def own_head(at):
        return jnp.sum(jnp.where(column == at, gates, 0.0), axis=1, keepdims=True)

    ingate = scale * own_head(at_ref[0])
    forget = scale * own_head(16 + at_ref[0]) + bias_ref[0]
    log_forget = -(jnp.maximum(-forget, 0.0) + jnp.log1p(jnp.exp(-jnp.abs(forget))))
    diagonal = lax.broadcasted_iota(jnp.int32, (16, 16), 0) == lax.broadcasted_iota(
        jnp.int32, (16, 16), 1
    )
    stabilizer = jnp.sum(jnp.where(diagonal, stabilizer_ref[...], 0.0), axis=1, keepdims=True)
    ceiling = jnp.maximum(log_forget + stabilizer, ingate)
    fresh = jnp.exp(ingate - ceiling)
    carried = jnp.exp(log_forget + stabilizer - ceiling)
    own = jnp.sum(query * key, axis=1, keepdims=True) * fresh
    recall = [
        jnp.sum(memory_ref[i] * query[i : i + 1], axis=1, keepdims=True) for i in range(16)
    ]
    recall = jnp.concatenate(recall + [jnp.zeros((128, 112), F32)], axis=1).T[:16]
    normalizer = normalizer_ref[...]
    denominator = own + carried * jnp.sum(normalizer * query, axis=1, keepdims=True)
    numerator = own * value + carried * recall
    readout = numerator / jnp.maximum(jnp.abs(denominator), jnp.exp(-ceiling))
    gated = (jax.nn.sigmoid(outgate) * readout).astype(BF)
    for i in range(copies_ref.shape[0]):
        copies_ref[i] = gated
    carried_ref[...] = jnp.broadcast_to(carried, carried_ref.shape)
    value_ref[...] = fresh * value
    key_ref[...] = key
    normalizer_out[...] = carried * normalizer + fresh * key
    stabilizer_out[...] = jnp.sum(jnp.where(diagonal, ceiling, 0.0), axis=0, keepdims=True)


def on_device(
    tokens,
    gain_first,
    gate_first,
    up_first,
    down_first,
    gain_mix,
    w_query,
    w_key,
    w_value,
    w_outgate,
    w_ingate,
    w_forget,
    forget_bias,
    memory,
    normalizer,
    stabilizer,
    w_project,
    gain_second,
    gate_second,
    up_second,
    down_second,
):
    pair = lax.axis_index("zp")
    core = lax.axis_index("c")
    at = lax.axis_index("tp")

    pair_at = jnp.reshape(pair, (1,)).astype(jnp.int32)
    core_at = jnp.reshape(core, (1,)).astype(jnp.int32)
    shard_at = jnp.reshape(at, (1,)).astype(jnp.int32)
    zero = jnp.zeros((1,), jnp.int32)
    wide_shape = jax.ShapeDtypeStruct((128, WIDE), BF)

    smem = pl.BlockSpec(memory_space=pltpu.SMEM)
    vmem = pl.BlockSpec(memory_space=pltpu.VMEM)
    packed = jax.ShapeDtypeStruct((HERE + WIDE, 128), BF)
    kept, sent = pl.pallas_call(
        prep_kernel,
        in_specs=[smem] + [vmem] * 4 + [pl.BlockSpec(memory_space=pl.ANY)] * 2,
        out_specs=(vmem, vmem),
        out_shape=(packed, packed),
        scratch_shapes=[pltpu.SemaphoreType.DMA((12,))],
        name="prep",
        compiler_params=pltpu.CompilerParams(vmem_limit_bytes=4 * 2**20),
    )(
        pair_at,
        tokens.reshape(8, NP, 2, 16, 128),
        gain_first.reshape(1, 128),
        gain_mix.reshape(1, 128),
        gain_second.reshape(1, 128),
        gate_first.T,
        up_first.T,
    )
    came = swap(sent)
    down_came = swap(down_first)
    heads = w_ingate.shape[1]
    middle = pack(
        [(i, 0, 128) for i in range(4)]
        + [(4, 0, heads), (5, 0, heads), (6, 0, 128), (7, FFL - 64, 64)],
        w_query,
        w_key,
        w_value,
        w_outgate,
        w_ingate.T,
        w_forget.T,
        w_project,
        down_second,
    )
    middle_came = swap(middle)
    last = pack(gate_up(0, 1) + [(2, 0, FFL - 64)], gate_second.T, up_second.T, down_second)
    last_came = swap(last)

    first_own, first_other = both_cores(kept), both_cores(came)
    down_own, down_other = both_cores(down_first), both_cores(down_came)
    middle_own, middle_other = both_cores(middle), both_cores(middle_came)
    last_own, last_other = both_cores(last), both_cores(last_came)

    shard = jax.ShapeDtypeStruct((1, 8, 512), BF)
    copied = jax.ShapeDtypeStruct((16, 8, 512), BF)
    wide, rows, gains = call(
        first_kernel, (wide_shape, copied, jax.ShapeDtypeStruct((3, 1, 512), F32)), 1
    )(core_at, first_own, first_other)
    came = half_step(wide, (((0, 0, FFL),), (down_own, down_other)))
    after_first, copies = call(residual_kernel(0.5), (shard, copied), 1)(shard_at, came, rows)
    copies = exchange(copies, "tp")

    mixed = call(mix_kernel, jax.ShapeDtypeStruct((128, MIX), BF))(
        copies, gains[1], middle_own, middle_other
    )
    summed = exchange(mixed.reshape(8, 16, MIX), "zq")
    small = jax.ShapeDtypeStruct((16, 128), F32)
    copies, carried, value, key, normalizer_new, stabilizer_new = call(
        cell_kernel,
        (jax.ShapeDtypeStruct((8, 16, 128), BF), small, small, small, small, jax.ShapeDtypeStruct((1, 16), F32)),
        2,
    )(
        shard_at,
        forget_bias,
        summed,
        memory.reshape(16, 128, 128),
        normalizer.reshape(16, 128),
        stabilizer.T,
    )
    memory_new = (
        carried[:, None, :1, None] * memory + value[:, None, :, None] * key[:, None, None, :]
    )
    normalizer_new = normalizer_new.reshape(normalizer.shape)
    stabilizer_new = stabilizer_new.T
    gated = exchange(copies, "zq")
    part = call(out_kernel(((0, 544, 128),)), jax.ShapeDtypeStruct((128, 512), BF))(
        gated, middle_own, middle_other
    )
    came = exchange(part.reshape(16, 8, 512), "tp")
    after_mix, copies = call(residual_kernel(1.0), (shard, copied), 1)(zero, came, after_first)
    copies = exchange(copies, "tp")

    wide = call(wide_kernel, wide_shape)(copies, gains[2], last_own, last_other)
    came = half_step(
        wide,
        (
            ((0, WIDE, FFL - 64), (1, 672, 64)),
            (last_own, last_other, middle_own, middle_other),
        ),
    )
    outgoing = call(last_kernel, jax.ShapeDtypeStruct((64, 8, 128), BF), 1)(
        pair_at, came, after_mix
    )
    came = exchange(outgoing, ("zp", "c", "tp"))
    came = came.reshape(NP, 2, 8, 16, 128).transpose(2, 0, 1, 3, 4)
    return (came.reshape(-1, 128), memory_new, normalizer_new, stabilizer_new)


def solution(mesh):
    kv, tp = mesh.shape["kv"], mesh.shape["tp"]
    finer = Mesh(mesh.devices.reshape(kv // (2 * NP), NP, 2, tp), ("zq", "zp", "c", "tp"))
    return jax.shard_map(
        on_device,
        mesh=finer,
        in_specs=(
            P(None, KV),
            P(KV),
            P(KV, "tp"),
            P(KV, "tp"),
            P("tp", KV),
            P(KV),
            P(KV, "tp"),
            P(KV, "tp"),
            P(KV, "tp"),
            P(KV, "tp"),
            P(KV, None),
            P(KV, None),
            P("tp"),
            P(KV, "tp", None, None),
            P(KV, "tp", None),
            P(KV, "tp"),
            P("tp", KV),
            P(KV),
            P(KV, "tp"),
            P(KV, "tp"),
            P("tp", KV),
        ),
        out_specs=(P(None, KV), P(KV, "tp", None, None), P(KV, "tp", None), P(KV, "tp")),
        check_vma=False,
    )
```

```python
import jax
import jax.numpy as jnp
from jax import lax
from jax.experimental import pallas as pl
from jax.experimental.pallas import tpu as pltpu
from jax.sharding import Mesh
from jax.sharding import PartitionSpec as P


D = 4096
EPSILON = 1e-06
NP = 2
KV = ("zq", "zp", "c")
BF = jnp.bfloat16
F32 = jnp.float32
FFL = 688
HEAD = 640
TAIL = 48
WIDE = 1408
MIX = 640
HERE = 272
NT_DIMS = (((1,), (1,)), ((), ()))


def swap(array):
    return lax.ppermute(array, "zp", [(0, 1), (1, 0)])


def both_cores(array):
    return lax.all_gather(array, "c")


def exchange(parts, axis):
    return lax.all_to_all(parts, axis, split_axis=0, concat_axis=0, tiled=True)


def pieces(gain):
    hi = gain.astype(BF)
    rest = gain - hi.astype(F32)
    mid = rest.astype(BF)
    low = (rest - mid.astype(F32)).astype(BF)
    return [hi, mid, low]


def gate_up(gate, up):
    return [
        (gate, 0, HEAD),
        (up, 0, HEAD),
        (gate, HEAD, TAIL),
        (gate, 0, 64 - TAIL),
        (up, HEAD, TAIL),
        (up, 0, 64 - TAIL),
    ]


def scaled_rows(x_ref, gain_ref):
    groups, rows, width = x_ref.shape
    x = x_ref[...].astype(F32).reshape(groups * rows, width)
    squares = jnp.sum(x * x, axis=1, keepdims=True)
    return (x * gain_ref[...]).astype(BF), squares


def put_squares(block, squares, at):
    hi = squares.astype(BF).astype(F32)
    low = squares - hi
    column = lax.broadcasted_iota(jnp.int32, block.shape, 1)
    return jnp.where(column == at, hi, jnp.where(column == at + 1, low, block))


def dot(a, b, dims=(((1,), (0,)), ((), ()))):
    return lax.dot_general(a, b, dims, preferred_element_type=F32)


def wide_kernel(x_ref, gain_ref, own_ref, other_ref, out_ref):
    scaled, squares = scaled_rows(x_ref, gain_ref)
    total = None
    for core in range(2):
        weight = jnp.concatenate([own_ref[core, :WIDE], other_ref[core, :WIDE]], axis=1)
        part = dot(scaled[:, 256 * core : 256 * (core + 1)], weight, NT_DIMS)
        total = part if total is None else total + part
    out_ref[:, : WIDE - 128] = total[:, : WIDE - 128].astype(BF)
    out_ref[:, WIDE - 128 :] = put_squares(total[:, WIDE - 128 :], squares, 112).astype(BF)


def prep_kernel(pair_ref, tokens_ref, first_ref, mix_ref, second_ref, gate_ref, up_ref, *refs):
    kept_ref, sent_ref, sems = refs
    copies = []
    for ref in (kept_ref, sent_ref):
        at = HERE
        for source, start, count in gate_up(gate_ref, up_ref):
            copy = pltpu.make_async_copy(
                source.at[pl.ds(start, count)], ref.at[pl.ds(at, count)], sems.at[len(copies)]
            )
            copy.start()
            copies.append(copy)
            at += count
    gains = []
    for ref in (first_ref, mix_ref, second_ref):
        gains += pieces(ref[...])
    rows = [g.astype(F32) for g in gains] + [jnp.zeros((7, 128), F32)]
    rows = jnp.concatenate(rows, axis=0).astype(BF)
    for ref, which in ((kept_ref, pair_ref[0]), (sent_ref, 1 - pair_ref[0])):
        for core in range(2):
            for group in range(8):
                at = 128 * core + 16 * group
                ref[at : at + 16] = tokens_ref[group, which, core]
        ref[256:HERE] = rows
    for copy in copies:
        copy.wait()


def pack_kernel(plan):
    def kernel(*refs):
        sources, out, sems = refs[:-2], refs[-2], refs[-1]
        started, at = [], 0
        for i, (source, start, count) in enumerate(plan):
            copy = pltpu.make_async_copy(
                sources[source].at[pl.ds(start, count)], out.at[pl.ds(at, count)], sems.at[i]
            )
            copy.start()
            started.append(copy)
            at += count
        for copy in started:
            copy.wait()

    return kernel


def pack(plan, *arrays):
    anywhere = pl.BlockSpec(memory_space=pl.ANY)
    return pl.pallas_call(
        pack_kernel(plan),
        in_specs=[pl.BlockSpec(memory_space=pltpu.HBM)] * len(arrays),
        out_specs=anywhere,
        out_shape=jax.ShapeDtypeStruct((sum(count for _, _, count in plan), 128), BF),
        scratch_shapes=[pltpu.SemaphoreType.DMA((len(plan),))],
        compiler_params=pltpu.CompilerParams(vmem_limit_bytes=2**20),
    )(*arrays)


def first_kernel(core_ref, own_ref, other_ref, out_ref, rows_ref, gains_ref):
    start = pl.multiple_of(128 * core_ref[0], 128)
    total, squares = None, None
    for core in range(2):
        x, gain = [], []
        for chip, here_ref in enumerate((own_ref, other_ref)):
            at = 128 * (2 * core + chip)
            block = here_ref[core, pl.ds(start, 128)]
            rows_ref[:, :, at : at + 128] = block.reshape(16, 8, 128)
            x.append(block.astype(F32))
            parts = here_ref[core, 256:HERE].astype(F32)
            for i in range(3):
                whole = (parts[3 * i : 3 * i + 1] + parts[3 * i + 1 : 3 * i + 2]) + parts[
                    3 * i + 2 : 3 * i + 3
                ]
                gains_ref[i, :, at : at + 128] = whole
                if i == 0:
                    gain.append(whole)
        x, gain = jnp.concatenate(x, axis=1), jnp.concatenate(gain, axis=1)
        square = jnp.sum(x * x, axis=1, keepdims=True)
        squares = square if squares is None else squares + square
        weight = jnp.concatenate([own_ref[core, HERE:], other_ref[core, HERE:]], axis=1)
        part = dot((x * gain).astype(BF), weight, NT_DIMS)
        total = part if total is None else total + part
    out_ref[:, : WIDE - 128] = total[:, : WIDE - 128].astype(BF)
    out_ref[:, WIDE - 128 :] = put_squares(total[:, WIDE - 128 :], squares, 112).astype(BF)


def mix_kernel(x_ref, gain_ref, own_ref, other_ref, out_ref):
    scaled, squares = scaled_rows(x_ref, gain_ref)
    for pair in range(2):
        total = None
        for core in range(2):
            columns = [
                jnp.concatenate(
                    [own_ref[core, 128 * m : 128 * (m + 1)], other_ref[core, 128 * m : 128 * (m + 1)]],
                    axis=0,
                )
                for m in (2 * pair, 2 * pair + 1)
            ]
            part = dot(scaled[:, 256 * core : 256 * (core + 1)], jnp.concatenate(columns, axis=1))
            total = part if total is None else total + part
        out_ref[:, 256 * pair : 256 * (pair + 1)] = total.astype(BF)
    total = None
    for core in range(2):
        weight = jnp.concatenate([own_ref[core, 512:544], other_ref[core, 512:544]], axis=1)
        weight = jnp.concatenate([weight, jnp.zeros((128 - weight.shape[0], 256), BF)], axis=0)
        part = dot(scaled[:, 256 * core : 256 * (core + 1)], weight, NT_DIMS)
        total = part if total is None else total + part
    out_ref[:, 512:] = put_squares(total, squares, 112).astype(BF)


def act_kernel(x_ref, out_ref):
    total = x_ref[0].astype(F32)
    for i in range(1, x_ref.shape[0]):
        total = total + x_ref[i].astype(F32)
    last = total[:, WIDE - 128 :]
    scale = lax.rsqrt((last[:, 112:113] + last[:, 113:114]) / D + EPSILON)

    def act(gate, up):
        gate, up = scale * gate, scale * up
        return (gate * jax.nn.sigmoid(gate) * up).astype(BF)

    head = act(total[:, :HEAD], total[:, HEAD : 2 * HEAD])
    tail = act(last, pltpu.roll(last, 64, 1))[:, :TAIL]
    for i in range(out_ref.shape[0]):
        out_ref[i, :, :HEAD] = head
        out_ref[i, :, HEAD:] = tail


def out_kernel(spans):
    def kernel(x_ref, *refs):
        out_ref = refs[-1]
        groups, rows, width = x_ref.shape
        x = x_ref[...].reshape(groups * rows, width)
        for core in range(2):
            columns = []
            for chip in range(2):
                blocks = [
                    refs[2 * source + chip][core, start : start + count]
                    for source, start, count in spans
                ]
                columns.append(blocks[0] if len(blocks) == 1 else jnp.concatenate(blocks, axis=0))
            part = dot(x, jnp.concatenate(columns, axis=1)).astype(BF)
            out_ref[:, 256 * core : 256 * (core + 1)] = part

    return kernel


def residual_kernel(factor):
    def kernel(at_ref, sum_ref, old_ref, new_ref, copies_ref):
        total = sum_ref[0].astype(F32)
        for i in range(1, sum_ref.shape[0]):
            total = total + sum_ref[i].astype(F32)
        new = (old_ref[at_ref[0]].astype(F32) + factor * total).astype(BF)
        new_ref[0] = new
        for i in range(copies_ref.shape[0]):
            copies_ref[i] = new

    return kernel


def last_kernel(at_ref, sum_ref, old_ref, out_ref):
    total = sum_ref[0].astype(F32)
    for i in range(1, sum_ref.shape[0]):
        total = total + sum_ref[i].astype(F32)
    new = (old_ref[0].astype(F32) + 0.5 * total).astype(BF)
    first = at_ref[0] == 0
    for core in range(2):
        own = new[:, 256 * core : 256 * core + 128]
        other = new[:, 256 * core + 128 : 256 * (core + 1)]
        blocks = (jnp.where(first, own, other), jnp.where(first, other, own))
        for pair in range(2):
            for i in range(16):
                out_ref[(2 * pair + core) * 16 + i] = blocks[pair]


def call(kernel, out_shapes, scalars=0):
    smem = pl.BlockSpec(memory_space=pltpu.SMEM)
    vmem = pl.BlockSpec(memory_space=pltpu.VMEM)

    def run(*args):
        return pl.pallas_call(
            kernel,
            in_specs=[smem] * scalars + [vmem] * (len(args) - scalars),
            out_specs=jax.tree.map(lambda s: vmem, out_shapes),
            out_shape=out_shapes,
            compiler_params=pltpu.CompilerParams(vmem_limit_bytes=12 * 2**20),
        )(*args)

    return run


def half_step(wide, down):
    came = exchange(wide.reshape(8, 16, WIDE), "zq")
    hidden = call(act_kernel, jax.ShapeDtypeStruct((8, 16, FFL), BF))(came)
    hidden = exchange(hidden, "zq")
    spans, weights = down
    part = call(out_kernel(spans), jax.ShapeDtypeStruct((128, 512), BF))(hidden, *weights)
    return exchange(part.reshape(16, 8, 512), "tp")


def cell_kernel(at_ref, bias_ref, x_ref, memory_ref, normalizer_ref, stabilizer_ref, *out_refs):
    copies_ref, carried_ref, value_ref, key_ref, normalizer_out, stabilizer_out = out_refs
    total = x_ref[0].astype(F32)
    for i in range(1, x_ref.shape[0]):
        total = total + x_ref[i].astype(F32)
    gates = total[:, 512:]
    scale = lax.rsqrt((gates[:, 112:113] + gates[:, 113:114]) / D + EPSILON)
    query, key, value, outgate = (
        (scale * total[:, 128 * i : 128 * (i + 1)]).astype(BF).astype(F32) for i in range(4)
    )
    key = key * 128 ** (-0.5)
    column = lax.broadcasted_iota(jnp.int32, gates.shape, 1)

    def own_head(at):
        return jnp.sum(jnp.where(column == at, gates, 0.0), axis=1, keepdims=True)

    ingate = scale * own_head(at_ref[0])
    forget = scale * own_head(16 + at_ref[0]) + bias_ref[0]
    log_forget = -(jnp.maximum(-forget, 0.0) + jnp.log1p(jnp.exp(-jnp.abs(forget))))
    diagonal = lax.broadcasted_iota(jnp.int32, (16, 16), 0) == lax.broadcasted_iota(
        jnp.int32, (16, 16), 1
    )
    stabilizer = jnp.sum(jnp.where(diagonal, stabilizer_ref[...], 0.0), axis=1, keepdims=True)
    ceiling = jnp.maximum(log_forget + stabilizer, ingate)
    fresh = jnp.exp(ingate - ceiling)
    carried = jnp.exp(log_forget + stabilizer - ceiling)
    own = jnp.sum(query * key, axis=1, keepdims=True) * fresh
    recall = [
        jnp.sum(memory_ref[i] * query[i : i + 1], axis=1, keepdims=True) for i in range(16)
    ]
    recall = jnp.concatenate(recall + [jnp.zeros((128, 112), F32)], axis=1).T[:16]
    normalizer = normalizer_ref[...]
    denominator = own + carried * jnp.sum(normalizer * query, axis=1, keepdims=True)
    numerator = own * value + carried * recall
    readout = numerator / jnp.maximum(jnp.abs(denominator), jnp.exp(-ceiling))
    gated = (jax.nn.sigmoid(outgate) * readout).astype(BF)
    for i in range(copies_ref.shape[0]):
        copies_ref[i] = gated
    carried_ref[...] = jnp.broadcast_to(carried, carried_ref.shape)
    value_ref[...] = fresh * value
    key_ref[...] = key
    normalizer_out[...] = carried * normalizer + fresh * key
    stabilizer_out[...] = jnp.sum(jnp.where(diagonal, ceiling, 0.0), axis=0, keepdims=True)


def on_device(
    tokens,
    gain_first,
    gate_first,
    up_first,
    down_first,
    gain_mix,
    w_query,
    w_key,
    w_value,
    w_outgate,
    w_ingate,
    w_forget,
    forget_bias,
    memory,
    normalizer,
    stabilizer,
    w_project,
    gain_second,
    gate_second,
    up_second,
    down_second,
):
    pair = lax.axis_index("zp")
    core = lax.axis_index("c")
    at = lax.axis_index("tp")

    pair_at = jnp.reshape(pair, (1,)).astype(jnp.int32)
    core_at = jnp.reshape(core, (1,)).astype(jnp.int32)
    shard_at = jnp.reshape(at, (1,)).astype(jnp.int32)
    zero = jnp.zeros((1,), jnp.int32)
    wide_shape = jax.ShapeDtypeStruct((128, WIDE), BF)

    smem = pl.BlockSpec(memory_space=pltpu.SMEM)
    vmem = pl.BlockSpec(memory_space=pltpu.VMEM)
    packed = jax.ShapeDtypeStruct((HERE + WIDE, 128), BF)
    kept, sent = pl.pallas_call(
        prep_kernel,
        in_specs=[smem] + [vmem] * 4 + [pl.BlockSpec(memory_space=pl.ANY)] * 2,
        out_specs=(vmem, vmem),
        out_shape=(packed, packed),
        scratch_shapes=[pltpu.SemaphoreType.DMA((12,))],
        name="prep",
        compiler_params=pltpu.CompilerParams(vmem_limit_bytes=4 * 2**20),
    )(
        pair_at,
        tokens.reshape(8, NP, 2, 16, 128),
        gain_first.reshape(1, 128),
        gain_mix.reshape(1, 128),
        gain_second.reshape(1, 128),
        gate_first.T,
        up_first.T,
    )
    came = swap(sent)
    heads = w_ingate.shape[1]
    middle = pack(
        [(i, 0, 128) for i in range(4)]
        + [(4, 0, heads), (5, 0, heads), (6, 0, 128), (7, FFL - 64, 64), (8, 0, FFL)],
        w_query,
        w_key,
        w_value,
        w_outgate,
        w_ingate.T,
        w_forget.T,
        w_project,
        down_second,
        down_first,
    )
    middle_came = swap(middle)
    last = pack(gate_up(0, 1) + [(2, 0, FFL - 64)], gate_second.T, up_second.T, down_second)
    last_came = swap(last)

    first_own, first_other = both_cores(kept), both_cores(came)
    middle_own, middle_other = both_cores(middle), both_cores(middle_came)
    last_own, last_other = both_cores(last), both_cores(last_came)

    shard = jax.ShapeDtypeStruct((1, 8, 512), BF)
    copied = jax.ShapeDtypeStruct((16, 8, 512), BF)
    wide, rows, gains = call(
        first_kernel, (wide_shape, copied, jax.ShapeDtypeStruct((3, 1, 512), F32)), 1
    )(core_at, first_own, first_other)
    came = half_step(wide, (((0, 736, FFL),), (middle_own, middle_other)))
    after_first, copies = call(residual_kernel(0.5), (shard, copied), 1)(shard_at, came, rows)
    copies = exchange(copies, "tp")

    mixed = call(mix_kernel, jax.ShapeDtypeStruct((128, MIX), BF))(
        copies, gains[1], middle_own, middle_other
    )
    summed = exchange(mixed.reshape(8, 16, MIX), "zq")
    small = jax.ShapeDtypeStruct((16, 128), F32)
    copies, carried, value, key, normalizer_new, stabilizer_new = call(
        cell_kernel,
        (jax.ShapeDtypeStruct((8, 16, 128), BF), small, small, small, small, jax.ShapeDtypeStruct((1, 16), F32)),
        2,
    )(
        shard_at,
        forget_bias,
        summed,
        memory.reshape(16, 128, 128),
        normalizer.reshape(16, 128),
        stabilizer.T,
    )
    memory_new = (
        carried[:, None, :1, None] * memory + value[:, None, :, None] * key[:, None, None, :]
    )
    normalizer_new = normalizer_new.reshape(normalizer.shape)
    stabilizer_new = stabilizer_new.T
    gated = exchange(copies, "zq")
    part = call(out_kernel(((0, 544, 128),)), jax.ShapeDtypeStruct((128, 512), BF))(
        gated, middle_own, middle_other
    )
    came = exchange(part.reshape(16, 8, 512), "tp")
    after_mix, copies = call(residual_kernel(1.0), (shard, copied), 1)(zero, came, after_first)
    copies = exchange(copies, "tp")

    wide = call(wide_kernel, wide_shape)(copies, gains[2], last_own, last_other)
    came = half_step(
        wide,
        (
            ((0, WIDE, FFL - 64), (1, 672, 64)),
            (last_own, last_other, middle_own, middle_other),
        ),
    )
    outgoing = call(last_kernel, jax.ShapeDtypeStruct((64, 8, 128), BF), 1)(
        pair_at, came, after_mix
    )
    came = exchange(outgoing, ("zp", "c", "tp"))
    came = came.reshape(NP, 2, 8, 16, 128).transpose(2, 0, 1, 3, 4)
    return (came.reshape(-1, 128), memory_new, normalizer_new, stabilizer_new)


def solution(mesh):
    kv, tp = mesh.shape["kv"], mesh.shape["tp"]
    finer = Mesh(mesh.devices.reshape(kv // (2 * NP), NP, 2, tp), ("zq", "zp", "c", "tp"))
    return jax.shard_map(
        on_device,
        mesh=finer,
        in_specs=(
            P(None, KV),
            P(KV),
            P(KV, "tp"),
            P(KV, "tp"),
            P("tp", KV),
            P(KV),
            P(KV, "tp"),
            P(KV, "tp"),
            P(KV, "tp"),
            P(KV, "tp"),
            P(KV, None),
            P(KV, None),
            P("tp"),
            P(KV, "tp", None, None),
            P(KV, "tp", None),
            P(KV, "tp"),
            P("tp", KV),
            P(KV),
            P(KV, "tp"),
            P(KV, "tp"),
            P("tp", KV),
        ),
        out_specs=(P(None, KV), P(KV, "tp", None, None), P(KV, "tp", None), P(KV, "tp")),
        check_vma=False,
    )
```

```python
import jax
import jax.numpy as jnp
from jax import lax
from jax.experimental import pallas as pl
from jax.experimental.pallas import tpu as pltpu
from jax.sharding import Mesh
from jax.sharding import PartitionSpec as P


D = 4096
EPSILON = 1e-06
NP = 2
KV = ("zq", "zp", "c")
BF = jnp.bfloat16
F32 = jnp.float32
FFL = 688
HEAD = 640
TAIL = 48
WIDE = 1408
MIX = 640
HERE = 272
NT_DIMS = (((1,), (1,)), ((), ()))


def swap(array):
    return lax.ppermute(array, "zp", [(0, 1), (1, 0)])


def both_cores(array):
    return lax.all_gather(array, "c")


def exchange(parts, axis):
    if axis == "zq":
        groups = [[2 * q + (role ^ (q >= 4)) for q in range(8)] for role in range(2)]
        return lax.all_to_all(
            parts, ("zq", "zp"), split_axis=0, concat_axis=0, axis_index_groups=groups, tiled=True
        )
    return lax.all_to_all(parts, axis, split_axis=0, concat_axis=0, tiled=True)


def pieces(gain):
    hi = gain.astype(BF)
    rest = gain - hi.astype(F32)
    mid = rest.astype(BF)
    low = (rest - mid.astype(F32)).astype(BF)
    return [hi, mid, low]


def gate_up(gate, up):
    return [
        (gate, 0, HEAD),
        (up, 0, HEAD),
        (gate, HEAD, TAIL),
        (gate, 0, 64 - TAIL),
        (up, HEAD, TAIL),
        (up, 0, 64 - TAIL),
    ]


def scaled_rows(x_ref, gain_ref):
    groups, rows, width = x_ref.shape
    x = x_ref[...].astype(F32).reshape(groups * rows, width)
    squares = jnp.sum(x * x, axis=1, keepdims=True)
    return (x * gain_ref[...]).astype(BF), squares


def put_squares(block, squares, at):
    hi = squares.astype(BF).astype(F32)
    low = squares - hi
    column = lax.broadcasted_iota(jnp.int32, block.shape, 1)
    return jnp.where(column == at, hi, jnp.where(column == at + 1, low, block))


def dot(a, b, dims=(((1,), (0,)), ((), ()))):
    return lax.dot_general(a, b, dims, preferred_element_type=F32)


def wide_kernel(x_ref, gain_ref, own_ref, other_ref, out_ref):
    scaled, squares = scaled_rows(x_ref, gain_ref)
    total = None
    for core in range(2):
        weight = jnp.concatenate([own_ref[core, :WIDE], other_ref[core, :WIDE]], axis=1)
        part = dot(scaled[:, 256 * core : 256 * (core + 1)], weight, NT_DIMS)
        total = part if total is None else total + part
    out_ref[:, : WIDE - 128] = total[:, : WIDE - 128].astype(BF)
    out_ref[:, WIDE - 128 :] = put_squares(total[:, WIDE - 128 :], squares, 112).astype(BF)


def prep_kernel(role_ref, tokens_ref, first_ref, mix_ref, second_ref, gate_ref, up_ref, *refs):
    kept_ref, sent_ref, sems = refs
    copies = []
    for ref in (kept_ref, sent_ref):
        at = HERE
        for source, start, count in gate_up(gate_ref, up_ref):
            copy = pltpu.make_async_copy(
                source.at[pl.ds(start, count)], ref.at[pl.ds(at, count)], sems.at[len(copies)]
            )
            copy.start()
            copies.append(copy)
            at += count
    gains = []
    for ref in (first_ref, mix_ref, second_ref):
        gains += pieces(ref[...])
    rows = [g.astype(F32) for g in gains] + [jnp.zeros((7, 128), F32)]
    rows = jnp.concatenate(rows, axis=0).astype(BF)
    for ref, which in ((kept_ref, role_ref[0]), (sent_ref, 1 - role_ref[0])):
        for core in range(2):
            for group in range(8):
                at = 128 * core + 16 * group
                ref[at : at + 16] = tokens_ref[group, which if group < 4 else 1 - which, core]
        ref[256:HERE] = rows
    for copy in copies:
        copy.wait()


def pack_kernel(plan):
    def kernel(*refs):
        sources, out, sems = refs[:-2], refs[-2], refs[-1]
        started, at = [], 0
        for i, (source, start, count) in enumerate(plan):
            copy = pltpu.make_async_copy(
                sources[source].at[pl.ds(start, count)], out.at[pl.ds(at, count)], sems.at[i]
            )
            copy.start()
            started.append(copy)
            at += count
        for copy in started:
            copy.wait()

    return kernel


def pack(plan, *arrays):
    anywhere = pl.BlockSpec(memory_space=pl.ANY)
    return pl.pallas_call(
        pack_kernel(plan),
        in_specs=[pl.BlockSpec(memory_space=pltpu.HBM)] * len(arrays),
        out_specs=anywhere,
        out_shape=jax.ShapeDtypeStruct((sum(count for _, _, count in plan), 128), BF),
        scratch_shapes=[pltpu.SemaphoreType.DMA((len(plan),))],
        compiler_params=pltpu.CompilerParams(vmem_limit_bytes=2**20),
    )(*arrays)


def first_kernel(core_ref, own_ref, other_ref, out_ref, rows_ref, gains_ref):
    start = pl.multiple_of(128 * core_ref[0], 128)
    total, squares = None, None
    for core in range(2):
        x, gain = [], []
        for chip, here_ref in enumerate((own_ref, other_ref)):
            at = 128 * (2 * core + chip)
            block = here_ref[core, pl.ds(start, 128)]
            rows_ref[:, :, at : at + 128] = block.reshape(16, 8, 128)
            x.append(block.astype(F32))
            parts = here_ref[core, 256:HERE].astype(F32)
            for i in range(3):
                whole = (parts[3 * i : 3 * i + 1] + parts[3 * i + 1 : 3 * i + 2]) + parts[
                    3 * i + 2 : 3 * i + 3
                ]
                gains_ref[i, :, at : at + 128] = whole
                if i == 0:
                    gain.append(whole)
        x, gain = jnp.concatenate(x, axis=1), jnp.concatenate(gain, axis=1)
        square = jnp.sum(x * x, axis=1, keepdims=True)
        squares = square if squares is None else squares + square
        weight = jnp.concatenate([own_ref[core, HERE:], other_ref[core, HERE:]], axis=1)
        part = dot((x * gain).astype(BF), weight, NT_DIMS)
        total = part if total is None else total + part
    out_ref[:, : WIDE - 128] = total[:, : WIDE - 128].astype(BF)
    out_ref[:, WIDE - 128 :] = put_squares(total[:, WIDE - 128 :], squares, 112).astype(BF)


def mix_kernel(x_ref, gain_ref, own_ref, other_ref, out_ref):
    scaled, squares = scaled_rows(x_ref, gain_ref)
    for pair in range(2):
        total = None
        for core in range(2):
            columns = [
                jnp.concatenate(
                    [own_ref[core, 128 * m : 128 * (m + 1)], other_ref[core, 128 * m : 128 * (m + 1)]],
                    axis=0,
                )
                for m in (2 * pair, 2 * pair + 1)
            ]
            part = dot(scaled[:, 256 * core : 256 * (core + 1)], jnp.concatenate(columns, axis=1))
            total = part if total is None else total + part
        out_ref[:, 256 * pair : 256 * (pair + 1)] = total.astype(BF)
    total = None
    for core in range(2):
        weight = jnp.concatenate([own_ref[core, 512:544], other_ref[core, 512:544]], axis=1)
        weight = jnp.concatenate([weight, jnp.zeros((128 - weight.shape[0], 256), BF)], axis=0)
        part = dot(scaled[:, 256 * core : 256 * (core + 1)], weight, NT_DIMS)
        total = part if total is None else total + part
    out_ref[:, 512:] = put_squares(total, squares, 112).astype(BF)


def act_kernel(x_ref, out_ref):
    total = x_ref[0].astype(F32)
    for i in range(1, x_ref.shape[0]):
        total = total + x_ref[i].astype(F32)
    last = total[:, WIDE - 128 :]
    scale = lax.rsqrt((last[:, 112:113] + last[:, 113:114]) / D + EPSILON)

    def act(gate, up):
        gate, up = scale * gate, scale * up
        return (gate * jax.nn.sigmoid(gate) * up).astype(BF)

    head = act(total[:, :HEAD], total[:, HEAD : 2 * HEAD])
    tail = act(last, pltpu.roll(last, 64, 1))[:, :TAIL]
    for i in range(out_ref.shape[0]):
        out_ref[i, :, :HEAD] = head
        out_ref[i, :, HEAD:] = tail


def out_kernel(spans):
    def kernel(x_ref, *refs):
        out_ref = refs[-1]
        groups, rows, width = x_ref.shape
        x = x_ref[...].reshape(groups * rows, width)
        for core in range(2):
            columns = []
            for chip in range(2):
                blocks = [
                    refs[2 * source + chip][core, start : start + count]
                    for source, start, count in spans
                ]
                columns.append(blocks[0] if len(blocks) == 1 else jnp.concatenate(blocks, axis=0))
            part = dot(x, jnp.concatenate(columns, axis=1)).astype(BF)
            out_ref[:, 256 * core : 256 * (core + 1)] = part

    return kernel


def residual_kernel(factor):
    def kernel(at_ref, sum_ref, old_ref, new_ref, copies_ref):
        total = sum_ref[0].astype(F32)
        for i in range(1, sum_ref.shape[0]):
            total = total + sum_ref[i].astype(F32)
        new = (old_ref[at_ref[0]].astype(F32) + factor * total).astype(BF)
        new_ref[0] = new
        for i in range(copies_ref.shape[0]):
            copies_ref[i] = new

    return kernel


def last_kernel(at_ref, sum_ref, old_ref, out_ref):
    total = sum_ref[0].astype(F32)
    for i in range(1, sum_ref.shape[0]):
        total = total + sum_ref[i].astype(F32)
    new = (old_ref[0].astype(F32) + 0.5 * total).astype(BF)
    first = at_ref[0] == 0
    for core in range(2):
        own = new[:, 256 * core : 256 * core + 128]
        other = new[:, 256 * core + 128 : 256 * (core + 1)]
        blocks = (jnp.where(first, own, other), jnp.where(first, other, own))
        for pair in range(2):
            for i in range(16):
                out_ref[(2 * pair + core) * 16 + i] = blocks[pair]


def unpack_kernel(upper_ref, came_ref, out_ref):
    for group in range(8):
        for role in range(2):
            base = role if group < 4 else 1 - role
            chip = upper_ref[0] if base == 0 else 1 - upper_ref[0]
            for core in range(2):
                out_ref[group, role, core] = came_ref[chip, core, group]


def call(kernel, out_shapes, scalars=0):
    smem = pl.BlockSpec(memory_space=pltpu.SMEM)
    vmem = pl.BlockSpec(memory_space=pltpu.VMEM)

    def run(*args):
        return pl.pallas_call(
            kernel,
            in_specs=[smem] * scalars + [vmem] * (len(args) - scalars),
            out_specs=jax.tree.map(lambda s: vmem, out_shapes),
            out_shape=out_shapes,
            compiler_params=pltpu.CompilerParams(vmem_limit_bytes=12 * 2**20),
        )(*args)

    return run


def half_step(wide, down):
    came = exchange(wide.reshape(8, 16, WIDE), "zq")
    hidden = call(act_kernel, jax.ShapeDtypeStruct((8, 16, FFL), BF))(came)
    hidden = exchange(hidden, "zq")
    spans, weights = down
    part = call(out_kernel(spans), jax.ShapeDtypeStruct((128, 512), BF))(hidden, *weights)
    return exchange(part.reshape(16, 8, 512), "tp")


def cell_kernel(at_ref, bias_ref, x_ref, memory_ref, normalizer_ref, stabilizer_ref, *out_refs):
    copies_ref, carried_ref, value_ref, key_ref, normalizer_out, stabilizer_out = out_refs
    total = x_ref[0].astype(F32)
    for i in range(1, x_ref.shape[0]):
        total = total + x_ref[i].astype(F32)
    gates = total[:, 512:]
    scale = lax.rsqrt((gates[:, 112:113] + gates[:, 113:114]) / D + EPSILON)
    query, key, value, outgate = (
        (scale * total[:, 128 * i : 128 * (i + 1)]).astype(BF).astype(F32) for i in range(4)
    )
    key = key * 128 ** (-0.5)
    column = lax.broadcasted_iota(jnp.int32, gates.shape, 1)

    def own_head(at):
        return jnp.sum(jnp.where(column == at, gates, 0.0), axis=1, keepdims=True)

    ingate = scale * own_head(at_ref[0])
    forget = scale * own_head(16 + at_ref[0]) + bias_ref[0]
    log_forget = -(jnp.maximum(-forget, 0.0) + jnp.log1p(jnp.exp(-jnp.abs(forget))))
    diagonal = lax.broadcasted_iota(jnp.int32, (16, 16), 0) == lax.broadcasted_iota(
        jnp.int32, (16, 16), 1
    )
    stabilizer = jnp.sum(jnp.where(diagonal, stabilizer_ref[...], 0.0), axis=1, keepdims=True)
    ceiling = jnp.maximum(log_forget + stabilizer, ingate)
    fresh = jnp.exp(ingate - ceiling)
    carried = jnp.exp(log_forget + stabilizer - ceiling)
    own = jnp.sum(query * key, axis=1, keepdims=True) * fresh
    recall = [
        jnp.sum(memory_ref[i] * query[i : i + 1], axis=1, keepdims=True) for i in range(16)
    ]
    recall = jnp.concatenate(recall + [jnp.zeros((128, 112), F32)], axis=1).T[:16]
    normalizer = normalizer_ref[...]
    denominator = own + carried * jnp.sum(normalizer * query, axis=1, keepdims=True)
    numerator = own * value + carried * recall
    readout = numerator / jnp.maximum(jnp.abs(denominator), jnp.exp(-ceiling))
    gated = (jax.nn.sigmoid(outgate) * readout).astype(BF)
    for i in range(copies_ref.shape[0]):
        copies_ref[i] = gated
    carried_ref[...] = jnp.broadcast_to(carried, carried_ref.shape)
    value_ref[...] = fresh * value
    key_ref[...] = key
    normalizer_out[...] = carried * normalizer + fresh * key
    stabilizer_out[...] = jnp.sum(jnp.where(diagonal, ceiling, 0.0), axis=0, keepdims=True)


def on_device(
    tokens,
    gain_first,
    gate_first,
    up_first,
    down_first,
    gain_mix,
    w_query,
    w_key,
    w_value,
    w_outgate,
    w_ingate,
    w_forget,
    forget_bias,
    memory,
    normalizer,
    stabilizer,
    w_project,
    gain_second,
    gate_second,
    up_second,
    down_second,
):
    pair = lax.axis_index("zp")
    core = lax.axis_index("c")
    at = lax.axis_index("tp")

    pair_at = jnp.reshape(pair, (1,)).astype(jnp.int32)
    upper = (lax.axis_index("zq") >= 4).astype(jnp.int32)
    upper_at = jnp.reshape(upper, (1,))
    role_at = pair_at + upper_at - 2 * pair_at * upper_at
    core_at = jnp.reshape(core, (1,)).astype(jnp.int32)
    shard_at = jnp.reshape(at, (1,)).astype(jnp.int32)
    zero = jnp.zeros((1,), jnp.int32)
    wide_shape = jax.ShapeDtypeStruct((128, WIDE), BF)

    smem = pl.BlockSpec(memory_space=pltpu.SMEM)
    vmem = pl.BlockSpec(memory_space=pltpu.VMEM)
    packed = jax.ShapeDtypeStruct((HERE + WIDE, 128), BF)
    kept, sent = pl.pallas_call(
        prep_kernel,
        in_specs=[smem] + [vmem] * 4 + [pl.BlockSpec(memory_space=pl.ANY)] * 2,
        out_specs=(vmem, vmem),
        out_shape=(packed, packed),
        scratch_shapes=[pltpu.SemaphoreType.DMA((12,))],
        name="prep",
        compiler_params=pltpu.CompilerParams(vmem_limit_bytes=4 * 2**20),
    )(
        role_at,
        tokens.reshape(8, NP, 2, 16, 128),
        gain_first.reshape(1, 128),
        gain_mix.reshape(1, 128),
        gain_second.reshape(1, 128),
        gate_first.T,
        up_first.T,
    )
    came = swap(sent)
    heads = w_ingate.shape[1]
    middle = pack(
        [(i, 0, 128) for i in range(4)]
        + [(4, 0, heads), (5, 0, heads), (6, 0, 128), (7, FFL - 64, 64), (8, 0, FFL)],
        w_query,
        w_key,
        w_value,
        w_outgate,
        w_ingate.T,
        w_forget.T,
        w_project,
        down_second,
        down_first,
    )
    middle_came = swap(middle)
    last = pack(gate_up(0, 1) + [(2, 0, FFL - 64)], gate_second.T, up_second.T, down_second)
    last_came = swap(last)

    first_own, first_other = both_cores(kept), both_cores(came)
    middle_own, middle_other = both_cores(middle), both_cores(middle_came)
    last_own, last_other = both_cores(last), both_cores(last_came)

    shard = jax.ShapeDtypeStruct((1, 8, 512), BF)
    copied = jax.ShapeDtypeStruct((16, 8, 512), BF)
    wide, rows, gains = call(
        first_kernel, (wide_shape, copied, jax.ShapeDtypeStruct((3, 1, 512), F32)), 1
    )(core_at, first_own, first_other)
    came = half_step(wide, (((0, 736, FFL),), (middle_own, middle_other)))
    after_first, copies = call(residual_kernel(0.5), (shard, copied), 1)(shard_at, came, rows)
    copies = exchange(copies, "tp")

    mixed = call(mix_kernel, jax.ShapeDtypeStruct((128, MIX), BF))(
        copies, gains[1], middle_own, middle_other
    )
    summed = exchange(mixed.reshape(8, 16, MIX), "zq")
    small = jax.ShapeDtypeStruct((16, 128), F32)
    copies, carried, value, key, normalizer_new, stabilizer_new = call(
        cell_kernel,
        (jax.ShapeDtypeStruct((8, 16, 128), BF), small, small, small, small, jax.ShapeDtypeStruct((1, 16), F32)),
        2,
    )(
        shard_at,
        forget_bias,
        summed,
        memory.reshape(16, 128, 128),
        normalizer.reshape(16, 128),
        stabilizer.T,
    )
    memory_new = (
        carried[:, None, :1, None] * memory + value[:, None, :, None] * key[:, None, None, :]
    )
    normalizer_new = normalizer_new.reshape(normalizer.shape)
    stabilizer_new = stabilizer_new.T
    gated = exchange(copies, "zq")
    part = call(out_kernel(((0, 544, 128),)), jax.ShapeDtypeStruct((128, 512), BF))(
        gated, middle_own, middle_other
    )
    came = exchange(part.reshape(16, 8, 512), "tp")
    after_mix, copies = call(residual_kernel(1.0), (shard, copied), 1)(zero, came, after_first)
    copies = exchange(copies, "tp")

    wide = call(wide_kernel, wide_shape)(copies, gains[2], last_own, last_other)
    came = half_step(
        wide,
        (
            ((0, WIDE, FFL - 64), (1, 672, 64)),
            (last_own, last_other, middle_own, middle_other),
        ),
    )
    outgoing = call(last_kernel, jax.ShapeDtypeStruct((64, 8, 128), BF), 1)(
        pair_at, came, after_mix
    )
    came = exchange(outgoing, ("zp", "c", "tp"))
    out = call(unpack_kernel, jax.ShapeDtypeStruct((8, NP, 2, 16, 128), BF), 1)(
        upper_at, came.reshape(NP, 2, 8, 16, 128)
    )
    return (out.reshape(-1, 128), memory_new, normalizer_new, stabilizer_new)


def solution(mesh):
    kv, tp = mesh.shape["kv"], mesh.shape["tp"]
    finer = Mesh(mesh.devices.reshape(kv // (2 * NP), NP, 2, tp), ("zq", "zp", "c", "tp"))
    return jax.shard_map(
        on_device,
        mesh=finer,
        in_specs=(
            P(None, KV),
            P(KV),
            P(KV, "tp"),
            P(KV, "tp"),
            P("tp", KV),
            P(KV),
            P(KV, "tp"),
            P(KV, "tp"),
            P(KV, "tp"),
            P(KV, "tp"),
            P(KV, None),
            P(KV, None),
            P("tp"),
            P(KV, "tp", None, None),
            P(KV, "tp", None),
            P(KV, "tp"),
            P("tp", KV),
            P(KV),
            P(KV, "tp"),
            P(KV, "tp"),
            P("tp", KV),
        ),
        out_specs=(P(None, KV), P(KV, "tp", None, None), P(KV, "tp", None), P(KV, "tp")),
        check_vma=False,
    )
```

```python
import jax
import jax.numpy as jnp
from jax import lax
from jax.experimental import pallas as pl
from jax.experimental.pallas import tpu as pltpu
from jax.sharding import Mesh
from jax.sharding import PartitionSpec as P


D = 4096
EPSILON = 1e-06
NP = 2
KV = ("zq", "zp", "c")
BF = jnp.bfloat16
F32 = jnp.float32
FFL = 688
HEAD = 640
TAIL = 48
WIDE = 1408
MIX = 640
HERE = 272
NT_DIMS = (((1,), (1,)), ((), ()))


def swap(array):
    return lax.ppermute(array, "zp", [(0, 1), (1, 0)])


def both_cores(array):
    return lax.all_gather(array, "c")


def exchange(parts, axis):
    if axis == "zq":
        groups = [[2 * q + (role ^ (q >= 4)) for q in range(8)] for role in range(2)]
        return lax.all_to_all(
            parts, ("zq", "zp"), split_axis=0, concat_axis=0, axis_index_groups=groups, tiled=True
        )
    return lax.all_to_all(parts, axis, split_axis=0, concat_axis=0, tiled=True)


def pieces(gain):
    hi = gain.astype(BF)
    rest = gain - hi.astype(F32)
    mid = rest.astype(BF)
    low = (rest - mid.astype(F32)).astype(BF)
    return [hi, mid, low]


def gate_up(gate, up):
    return [
        (gate, 0, HEAD),
        (up, 0, HEAD),
        (gate, HEAD, TAIL),
        (gate, 0, 64 - TAIL),
        (up, HEAD, TAIL),
        (up, 0, 64 - TAIL),
    ]


def scaled_rows(x_ref, gain):
    groups, rows, width = x_ref.shape
    x = x_ref[...].astype(F32).reshape(groups * rows, width)
    squares = jnp.sum(x * x, axis=1, keepdims=True)
    return (x * gain).astype(BF), squares


def put_squares(block, squares, at):
    hi = squares.astype(BF).astype(F32)
    low = squares - hi
    column = lax.broadcasted_iota(jnp.int32, block.shape, 1)
    return jnp.where(column == at, hi, jnp.where(column == at + 1, low, block))


def dot(a, b, dims=(((1,), (0,)), ((), ()))):
    return lax.dot_general(a, b, dims, preferred_element_type=F32)


def wide_kernel(x_ref, gain_ref, own_ref, other_ref, out_ref):
    scaled, squares = scaled_rows(x_ref, gain_ref[2])
    total = None
    for core in range(2):
        weight = jnp.concatenate([own_ref[core, :WIDE], other_ref[core, :WIDE]], axis=1)
        part = dot(scaled[:, 256 * core : 256 * (core + 1)], weight, NT_DIMS)
        total = part if total is None else total + part
    out_ref[:, : WIDE - 128] = total[:, : WIDE - 128].astype(BF)
    out_ref[:, WIDE - 128 :] = put_squares(total[:, WIDE - 128 :], squares, 112).astype(BF)


def prep_kernel(role_ref, tokens_ref, first_ref, mix_ref, second_ref, gate_ref, up_ref, *refs):
    kept_ref, sent_ref, sems = refs
    copies = []
    for ref in (kept_ref, sent_ref):
        at = HERE
        for source, start, count in gate_up(gate_ref, up_ref):
            copy = pltpu.make_async_copy(
                source.at[pl.ds(start, count)], ref.at[pl.ds(at, count)], sems.at[len(copies)]
            )
            copy.start()
            copies.append(copy)
            at += count
    gains = []
    for ref in (first_ref, mix_ref, second_ref):
        gains += pieces(ref[...])
    rows = [g.astype(F32) for g in gains] + [jnp.zeros((7, 128), F32)]
    rows = jnp.concatenate(rows, axis=0).astype(BF)
    for ref, which in ((kept_ref, role_ref[0]), (sent_ref, 1 - role_ref[0])):
        for core in range(2):
            for group in range(8):
                at = 128 * core + 16 * group
                ref[at : at + 16] = tokens_ref[group, which if group < 4 else 1 - which, core]
        ref[256:HERE] = rows
    for copy in copies:
        copy.wait()


def pack_kernel(plan):
    def kernel(*refs):
        sources, out, sems = refs[:-2], refs[-2], refs[-1]
        started, at = [], 0
        for i, (source, start, count) in enumerate(plan):
            copy = pltpu.make_async_copy(
                sources[source].at[pl.ds(start, count)], out.at[pl.ds(at, count)], sems.at[i]
            )
            copy.start()
            started.append(copy)
            at += count
        for copy in started:
            copy.wait()

    return kernel


def pack(plan, *arrays):
    anywhere = pl.BlockSpec(memory_space=pl.ANY)
    return pl.pallas_call(
        pack_kernel(plan),
        in_specs=[pl.BlockSpec(memory_space=pltpu.HBM)] * len(arrays),
        out_specs=anywhere,
        out_shape=jax.ShapeDtypeStruct((sum(count for _, _, count in plan), 128), BF),
        scratch_shapes=[pltpu.SemaphoreType.DMA((len(plan),))],
        compiler_params=pltpu.CompilerParams(vmem_limit_bytes=2**20),
    )(*arrays)


def first_kernel(core_ref, own_ref, other_ref, out_ref, rows_ref, gains_ref):
    start = pl.multiple_of(128 * core_ref[0], 128)
    total, squares = None, None
    for core in range(2):
        x, gain = [], []
        for chip, here_ref in enumerate((own_ref, other_ref)):
            at = 128 * (2 * core + chip)
            block = here_ref[core, pl.ds(start, 128)]
            rows_ref[:, :, at : at + 128] = block.reshape(16, 8, 128)
            x.append(block.astype(F32))
            parts = here_ref[core, 256:HERE].astype(F32)
            for i in range(3):
                whole = (parts[3 * i : 3 * i + 1] + parts[3 * i + 1 : 3 * i + 2]) + parts[
                    3 * i + 2 : 3 * i + 3
                ]
                gains_ref[i, :, at : at + 128] = whole
                if i == 0:
                    gain.append(whole)
        x, gain = jnp.concatenate(x, axis=1), jnp.concatenate(gain, axis=1)
        square = jnp.sum(x * x, axis=1, keepdims=True)
        squares = square if squares is None else squares + square
        weight = jnp.concatenate([own_ref[core, HERE:], other_ref[core, HERE:]], axis=1)
        part = dot((x * gain).astype(BF), weight, NT_DIMS)
        total = part if total is None else total + part
    out_ref[:, : WIDE - 128] = total[:, : WIDE - 128].astype(BF)
    out_ref[:, WIDE - 128 :] = put_squares(total[:, WIDE - 128 :], squares, 112).astype(BF)


def mix_kernel(x_ref, gain_ref, own_ref, other_ref, out_ref):
    scaled, squares = scaled_rows(x_ref, gain_ref[1])
    for pair in range(2):
        total = None
        for core in range(2):
            columns = [
                jnp.concatenate(
                    [own_ref[core, 128 * m : 128 * (m + 1)], other_ref[core, 128 * m : 128 * (m + 1)]],
                    axis=0,
                )
                for m in (2 * pair, 2 * pair + 1)
            ]
            part = dot(scaled[:, 256 * core : 256 * (core + 1)], jnp.concatenate(columns, axis=1))
            total = part if total is None else total + part
        out_ref[:, 256 * pair : 256 * (pair + 1)] = total.astype(BF)
    total = None
    for core in range(2):
        weight = jnp.concatenate([own_ref[core, 512:544], other_ref[core, 512:544]], axis=1)
        weight = jnp.concatenate([weight, jnp.zeros((128 - weight.shape[0], 256), BF)], axis=0)
        part = dot(scaled[:, 256 * core : 256 * (core + 1)], weight, NT_DIMS)
        total = part if total is None else total + part
    out_ref[:, 512:] = put_squares(total, squares, 112).astype(BF)


def act_kernel(x_ref, out_ref):
    total = x_ref[0].astype(F32)
    for i in range(1, x_ref.shape[0]):
        total = total + x_ref[i].astype(F32)
    last = total[:, WIDE - 128 :]
    scale = lax.rsqrt((last[:, 112:113] + last[:, 113:114]) / D + EPSILON)

    def act(gate, up):
        gate, up = scale * gate, scale * up
        return (gate * jax.nn.sigmoid(gate) * up).astype(BF)

    head = act(total[:, :HEAD], total[:, HEAD : 2 * HEAD])
    tail = act(last, pltpu.roll(last, 64, 1))[:, :TAIL]
    for i in range(out_ref.shape[0]):
        out_ref[i, :, :HEAD] = head
        out_ref[i, :, HEAD:] = tail


def out_kernel(spans):
    def kernel(x_ref, *refs):
        out_ref = refs[-1]
        groups, rows, width = x_ref.shape
        x = x_ref[...].reshape(groups * rows, width)
        for core in range(2):
            columns = []
            for chip in range(2):
                blocks = [
                    refs[2 * source + chip][core, start : start + count]
                    for source, start, count in spans
                ]
                columns.append(blocks[0] if len(blocks) == 1 else jnp.concatenate(blocks, axis=0))
            part = dot(x, jnp.concatenate(columns, axis=1)).astype(BF)
            out_ref[:, 256 * core : 256 * (core + 1)] = part

    return kernel


def residual_kernel(factor):
    def kernel(at_ref, sum_ref, old_ref, new_ref, copies_ref):
        total = sum_ref[0].astype(F32)
        for i in range(1, sum_ref.shape[0]):
            total = total + sum_ref[i].astype(F32)
        new = (old_ref[at_ref[0]].astype(F32) + factor * total).astype(BF)
        new_ref[0] = new
        for i in range(copies_ref.shape[0]):
            copies_ref[i] = new

    return kernel


def last_kernel(at_ref, sum_ref, old_ref, out_ref):
    total = sum_ref[0].astype(F32)
    for i in range(1, sum_ref.shape[0]):
        total = total + sum_ref[i].astype(F32)
    new = (old_ref[0].astype(F32) + 0.5 * total).astype(BF)
    first = at_ref[0] == 0
    for core in range(2):
        own = new[:, 256 * core : 256 * core + 128]
        other = new[:, 256 * core + 128 : 256 * (core + 1)]
        blocks = (jnp.where(first, own, other), jnp.where(first, other, own))
        for pair in range(2):
            for i in range(16):
                out_ref[(2 * pair + core) * 16 + i] = blocks[pair]


def unpack_kernel(upper_ref, came_ref, out_ref):
    for group in range(8):
        for role in range(2):
            base = role if group < 4 else 1 - role
            chip = upper_ref[0] if base == 0 else 1 - upper_ref[0]
            for core in range(2):
                out_ref[group, role, core] = came_ref[chip, core, group]


def call(kernel, out_shapes, scalars=0):
    smem = pl.BlockSpec(memory_space=pltpu.SMEM)
    vmem = pl.BlockSpec(memory_space=pltpu.VMEM)

    def run(*args):
        return pl.pallas_call(
            kernel,
            in_specs=[smem] * scalars + [vmem] * (len(args) - scalars),
            out_specs=jax.tree.map(lambda s: vmem, out_shapes),
            out_shape=out_shapes,
            compiler_params=pltpu.CompilerParams(vmem_limit_bytes=12 * 2**20),
        )(*args)

    return run


def half_step(wide, down):
    came = exchange(wide.reshape(8, 16, WIDE), "zq")
    hidden = call(act_kernel, jax.ShapeDtypeStruct((8, 16, FFL), BF))(came)
    hidden = exchange(hidden, "zq")
    spans, weights = down
    part = call(out_kernel(spans), jax.ShapeDtypeStruct((128, 512), BF))(hidden, *weights)
    return exchange(part.reshape(16, 8, 512), "tp")


def cell_kernel(at_ref, bias_ref, x_ref, memory_ref, normalizer_ref, stabilizer_ref, *out_refs):
    copies_ref, carried_ref, value_ref, key_ref, normalizer_out, stabilizer_out = out_refs
    total = x_ref[0].astype(F32)
    for i in range(1, x_ref.shape[0]):
        total = total + x_ref[i].astype(F32)
    gates = total[:, 512:]
    scale = lax.rsqrt((gates[:, 112:113] + gates[:, 113:114]) / D + EPSILON)
    query, key, value, outgate = (
        (scale * total[:, 128 * i : 128 * (i + 1)]).astype(BF).astype(F32) for i in range(4)
    )
    key = key * 128 ** (-0.5)
    column = lax.broadcasted_iota(jnp.int32, gates.shape, 1)

    def own_head(at):
        return jnp.sum(jnp.where(column == at, gates, 0.0), axis=1, keepdims=True)

    ingate = scale * own_head(at_ref[0])
    forget = scale * own_head(16 + at_ref[0]) + bias_ref[0]
    log_forget = -(jnp.maximum(-forget, 0.0) + jnp.log1p(jnp.exp(-jnp.abs(forget))))
    diagonal = lax.broadcasted_iota(jnp.int32, (16, 16), 0) == lax.broadcasted_iota(
        jnp.int32, (16, 16), 1
    )
    stabilizer = jnp.sum(jnp.where(diagonal, stabilizer_ref[...], 0.0), axis=1, keepdims=True)
    ceiling = jnp.maximum(log_forget + stabilizer, ingate)
    fresh = jnp.exp(ingate - ceiling)
    carried = jnp.exp(log_forget + stabilizer - ceiling)
    own = jnp.sum(query * key, axis=1, keepdims=True) * fresh
    recall = [
        jnp.sum(memory_ref[i] * query[i : i + 1], axis=1, keepdims=True) for i in range(16)
    ]
    recall = jnp.concatenate(recall + [jnp.zeros((128, 112), F32)], axis=1).T[:16]
    normalizer = normalizer_ref[...]
    denominator = own + carried * jnp.sum(normalizer * query, axis=1, keepdims=True)
    numerator = own * value + carried * recall
    readout = numerator / jnp.maximum(jnp.abs(denominator), jnp.exp(-ceiling))
    gated = (jax.nn.sigmoid(outgate) * readout).astype(BF)
    for i in range(copies_ref.shape[0]):
        copies_ref[i] = gated
    carried_ref[...] = jnp.broadcast_to(carried, carried_ref.shape)
    value_ref[...] = fresh * value
    key_ref[...] = key
    normalizer_out[...] = carried * normalizer + fresh * key
    stabilizer_out[...] = jnp.sum(jnp.where(diagonal, ceiling, 0.0), axis=0, keepdims=True)


def on_device(
    tokens,
    gain_first,
    gate_first,
    up_first,
    down_first,
    gain_mix,
    w_query,
    w_key,
    w_value,
    w_outgate,
    w_ingate,
    w_forget,
    forget_bias,
    memory,
    normalizer,
    stabilizer,
    w_project,
    gain_second,
    gate_second,
    up_second,
    down_second,
):
    pair = lax.axis_index("zp")
    core = lax.axis_index("c")
    at = lax.axis_index("tp")

    pair_at = jnp.reshape(pair, (1,)).astype(jnp.int32)
    upper = (lax.axis_index("zq") >= 4).astype(jnp.int32)
    upper_at = jnp.reshape(upper, (1,))
    role_at = pair_at + upper_at - 2 * pair_at * upper_at
    core_at = jnp.reshape(core, (1,)).astype(jnp.int32)
    shard_at = jnp.reshape(at, (1,)).astype(jnp.int32)
    zero = jnp.zeros((1,), jnp.int32)
    wide_shape = jax.ShapeDtypeStruct((128, WIDE), BF)

    smem = pl.BlockSpec(memory_space=pltpu.SMEM)
    vmem = pl.BlockSpec(memory_space=pltpu.VMEM)
    packed = jax.ShapeDtypeStruct((HERE + WIDE, 128), BF)
    kept, sent = pl.pallas_call(
        prep_kernel,
        in_specs=[smem] + [vmem] * 4 + [pl.BlockSpec(memory_space=pl.ANY)] * 2,
        out_specs=(vmem, vmem),
        out_shape=(packed, packed),
        scratch_shapes=[pltpu.SemaphoreType.DMA((12,))],
        name="prep",
        compiler_params=pltpu.CompilerParams(vmem_limit_bytes=4 * 2**20),
    )(
        role_at,
        tokens.reshape(8, NP, 2, 16, 128),
        gain_first.reshape(1, 128),
        gain_mix.reshape(1, 128),
        gain_second.reshape(1, 128),
        gate_first.T,
        up_first.T,
    )
    came = swap(sent)
    heads = w_ingate.shape[1]
    middle = pack(
        [(i, 0, 128) for i in range(4)]
        + [(4, 0, heads), (5, 0, heads), (6, 0, 128), (7, FFL - 64, 64), (8, 0, FFL)],
        w_query,
        w_key,
        w_value,
        w_outgate,
        w_ingate.T,
        w_forget.T,
        w_project,
        down_second,
        down_first,
    )
    middle_came = swap(middle)
    last = pack(gate_up(0, 1) + [(2, 0, FFL - 64)], gate_second.T, up_second.T, down_second)
    last_came = swap(last)

    first_own, first_other = both_cores(kept), both_cores(came)
    middle_own, middle_other = both_cores(middle), both_cores(middle_came)
    last_own, last_other = both_cores(last), both_cores(last_came)

    shard = jax.ShapeDtypeStruct((1, 8, 512), BF)
    copied = jax.ShapeDtypeStruct((16, 8, 512), BF)
    wide, rows, gains = call(
        first_kernel, (wide_shape, copied, jax.ShapeDtypeStruct((3, 1, 512), F32)), 1
    )(core_at, first_own, first_other)
    came = half_step(wide, (((0, 736, FFL),), (middle_own, middle_other)))
    after_first, copies = call(residual_kernel(0.5), (shard, copied), 1)(shard_at, came, rows)
    copies = exchange(copies, "tp")

    mixed = call(mix_kernel, jax.ShapeDtypeStruct((128, MIX), BF))(
        copies, gains, middle_own, middle_other
    )
    summed = exchange(mixed.reshape(8, 16, MIX), "zq")
    small = jax.ShapeDtypeStruct((16, 128), F32)
    copies, carried, value, key, normalizer_new, stabilizer_new = call(
        cell_kernel,
        (jax.ShapeDtypeStruct((8, 16, 128), BF), small, small, small, small, jax.ShapeDtypeStruct((1, 16), F32)),
        2,
    )(
        shard_at,
        forget_bias,
        summed,
        memory.reshape(16, 128, 128),
        normalizer.reshape(16, 128),
        stabilizer.T,
    )
    memory_new = (
        carried[:, None, :1, None] * memory + value[:, None, :, None] * key[:, None, None, :]
    )
    normalizer_new = normalizer_new.reshape(normalizer.shape)
    stabilizer_new = stabilizer_new.T
    gated = exchange(copies, "zq")
    part = call(out_kernel(((0, 544, 128),)), jax.ShapeDtypeStruct((128, 512), BF))(
        gated, middle_own, middle_other
    )
    came = exchange(part.reshape(16, 8, 512), "tp")
    after_mix, copies = call(residual_kernel(1.0), (shard, copied), 1)(zero, came, after_first)
    copies = exchange(copies, "tp")

    wide = call(wide_kernel, wide_shape)(copies, gains, last_own, last_other)
    came = half_step(
        wide,
        (
            ((0, WIDE, FFL - 64), (1, 672, 64)),
            (last_own, last_other, middle_own, middle_other),
        ),
    )
    outgoing = call(last_kernel, jax.ShapeDtypeStruct((64, 8, 128), BF), 1)(
        pair_at, came, after_mix
    )
    came = exchange(outgoing, ("zp", "c", "tp"))
    out = call(unpack_kernel, jax.ShapeDtypeStruct((8, NP, 2, 16, 128), BF), 1)(
        upper_at, came.reshape(NP, 2, 8, 16, 128)
    )
    return (out.reshape(-1, 128), memory_new, normalizer_new, stabilizer_new)


def solution(mesh):
    kv, tp = mesh.shape["kv"], mesh.shape["tp"]
    finer = Mesh(mesh.devices.reshape(kv // (2 * NP), NP, 2, tp), ("zq", "zp", "c", "tp"))
    return jax.shard_map(
        on_device,
        mesh=finer,
        in_specs=(
            P(None, KV),
            P(KV),
            P(KV, "tp"),
            P(KV, "tp"),
            P("tp", KV),
            P(KV),
            P(KV, "tp"),
            P(KV, "tp"),
            P(KV, "tp"),
            P(KV, "tp"),
            P(KV, None),
            P(KV, None),
            P("tp"),
            P(KV, "tp", None, None),
            P(KV, "tp", None),
            P(KV, "tp"),
            P("tp", KV),
            P(KV),
            P(KV, "tp"),
            P(KV, "tp"),
            P("tp", KV),
        ),
        out_specs=(P(None, KV), P(KV, "tp", None, None), P(KV, "tp", None), P(KV, "tp")),
        check_vma=False,
    )
```

```python
import jax
import jax.numpy as jnp
from jax import lax
from jax.experimental import pallas as pl
from jax.experimental.pallas import tpu as pltpu
from jax.sharding import Mesh
from jax.sharding import PartitionSpec as P


D = 4096
EPSILON = 1e-06
NP = 2
KV = ("zq", "zp", "c")
BF = jnp.bfloat16
F32 = jnp.float32
FFL = 688
HEAD = 640
TAIL = 48
WIDE = 1408
MIX = 640
HERE = 272
NT_DIMS = (((1,), (1,)), ((), ()))


def swap(array):
    return lax.ppermute(array, "zp", [(0, 1), (1, 0)])


def both_cores(array):
    return lax.all_gather(array, "c")


def exchange(parts, axis):
    if axis == "zq":
        groups = [[2 * q + (role ^ (q >= 4)) for q in range(8)] for role in range(2)]
        return lax.all_to_all(
            parts, ("zq", "zp"), split_axis=0, concat_axis=0, axis_index_groups=groups, tiled=True
        )
    return lax.all_to_all(parts, axis, split_axis=0, concat_axis=0, tiled=True)


def pieces(gain):
    hi = gain.astype(BF)
    rest = gain - hi.astype(F32)
    mid = rest.astype(BF)
    low = (rest - mid.astype(F32)).astype(BF)
    return [hi, mid, low]


def gate_up(gate, up):
    return [
        (gate, 0, HEAD),
        (up, 0, HEAD),
        (gate, HEAD, TAIL),
        (gate, 0, 64 - TAIL),
        (up, HEAD, TAIL),
        (up, 0, 64 - TAIL),
    ]


def scaled_rows(x_ref, gain):
    groups, rows, width = x_ref.shape
    x = x_ref[...].astype(F32).reshape(groups * rows, width)
    squares = jnp.sum(x * x, axis=1, keepdims=True)
    return (x * gain).astype(BF), squares


def put_squares(block, squares, at):
    hi = squares.astype(BF).astype(F32)
    low = squares - hi
    column = lax.broadcasted_iota(jnp.int32, block.shape, 1)
    return jnp.where(column == at, hi, jnp.where(column == at + 1, low, block))


def dot(a, b, dims=(((1,), (0,)), ((), ()))):
    return lax.dot_general(a, b, dims, preferred_element_type=F32)


def wide_kernel(x_ref, gain_ref, own_ref, other_ref, out_ref):
    scaled, squares = scaled_rows(x_ref, gain_ref[2])
    total = None
    for core in range(2):
        weight = jnp.concatenate([own_ref[core, :WIDE], other_ref[core, :WIDE]], axis=1)
        part = dot(scaled[:, 256 * core : 256 * (core + 1)], weight, NT_DIMS)
        total = part if total is None else total + part
    out_ref[:, : WIDE - 128] = total[:, : WIDE - 128].astype(BF)
    out_ref[:, WIDE - 128 :] = put_squares(total[:, WIDE - 128 :], squares, 112).astype(BF)


def prep_kernel(role_ref, tokens_ref, first_ref, mix_ref, second_ref, gate_ref, up_ref, *refs):
    kept_ref, sent_ref, sems = refs
    copies = []
    for ref in (kept_ref, sent_ref):
        at = HERE
        for source, start, count in gate_up(gate_ref, up_ref):
            copy = pltpu.make_async_copy(
                source.at[pl.ds(start, count)], ref.at[pl.ds(at, count)], sems.at[len(copies)]
            )
            copy.start()
            copies.append(copy)
            at += count
    gains = []
    for ref in (first_ref, mix_ref, second_ref):
        gains += pieces(ref[...])
    rows = [g.astype(F32) for g in gains] + [jnp.zeros((7, 128), F32)]
    rows = jnp.concatenate(rows, axis=0).astype(BF)
    for ref, which in ((kept_ref, role_ref[0]), (sent_ref, 1 - role_ref[0])):
        for core in range(2):
            for group in range(8):
                at = 128 * core + 16 * group
                ref[at : at + 16] = tokens_ref[group, which if group < 4 else 1 - which, core]
        ref[256:HERE] = rows
    for copy in copies:
        copy.wait()


def pack_kernel(plan):
    def kernel(*refs):
        sources, out, sems = refs[:-2], refs[-2], refs[-1]
        started, at = [], 0
        for i, (source, start, count) in enumerate(plan):
            copy = pltpu.make_async_copy(
                sources[source].at[pl.ds(start, count)], out.at[pl.ds(at, count)], sems.at[i]
            )
            copy.start()
            started.append(copy)
            at += count
        for copy in started:
            copy.wait()

    return kernel


def pack(plan, *arrays):
    anywhere = pl.BlockSpec(memory_space=pl.ANY)
    return pl.pallas_call(
        pack_kernel(plan),
        in_specs=[pl.BlockSpec(memory_space=pltpu.HBM)] * len(arrays),
        out_specs=anywhere,
        out_shape=jax.ShapeDtypeStruct((sum(count for _, _, count in plan), 128), BF),
        scratch_shapes=[pltpu.SemaphoreType.DMA((len(plan),))],
        compiler_params=pltpu.CompilerParams(vmem_limit_bytes=2**20),
    )(*arrays)


def first_kernel(core_ref, own_ref, other_ref, out_ref, rows_ref, gains_ref):
    start = pl.multiple_of(128 * core_ref[0], 128)
    total, squares = None, None
    for core in range(2):
        x, gain = [], []
        for chip, here_ref in enumerate((own_ref, other_ref)):
            at = 128 * (2 * core + chip)
            block = here_ref[core, pl.ds(start, 128)]
            rows_ref[:, :, at : at + 128] = block.reshape(16, 8, 128)
            x.append(block.astype(F32))
            parts = here_ref[core, 256:HERE].astype(F32)
            for i in range(3):
                whole = (parts[3 * i : 3 * i + 1] + parts[3 * i + 1 : 3 * i + 2]) + parts[
                    3 * i + 2 : 3 * i + 3
                ]
                gains_ref[i, :, at : at + 128] = whole
                if i == 0:
                    gain.append(whole)
        x, gain = jnp.concatenate(x, axis=1), jnp.concatenate(gain, axis=1)
        square = jnp.sum(x * x, axis=1, keepdims=True)
        squares = square if squares is None else squares + square
        weight = jnp.concatenate([own_ref[core, HERE:], other_ref[core, HERE:]], axis=1)
        part = dot((x * gain).astype(BF), weight, NT_DIMS)
        total = part if total is None else total + part
    out_ref[:, : WIDE - 128] = total[:, : WIDE - 128].astype(BF)
    out_ref[:, WIDE - 128 :] = put_squares(total[:, WIDE - 128 :], squares, 112).astype(BF)


def mix_kernel(x_ref, gain_ref, own_ref, other_ref, out_ref):
    scaled, squares = scaled_rows(x_ref, gain_ref[1])
    for pair in range(2):
        total = None
        for core in range(2):
            columns = [
                jnp.concatenate(
                    [own_ref[core, 128 * m : 128 * (m + 1)], other_ref[core, 128 * m : 128 * (m + 1)]],
                    axis=0,
                )
                for m in (2 * pair, 2 * pair + 1)
            ]
            part = dot(scaled[:, 256 * core : 256 * (core + 1)], jnp.concatenate(columns, axis=1))
            total = part if total is None else total + part
        out_ref[:, 256 * pair : 256 * (pair + 1)] = total.astype(BF)
    total = None
    for core in range(2):
        weight = jnp.concatenate([own_ref[core, 512:544], other_ref[core, 512:544]], axis=1)
        weight = jnp.concatenate([weight, jnp.zeros((128 - weight.shape[0], 256), BF)], axis=0)
        part = dot(scaled[:, 256 * core : 256 * (core + 1)], weight, NT_DIMS)
        total = part if total is None else total + part
    out_ref[:, 512:] = put_squares(total, squares, 112).astype(BF)


def act_kernel(x_ref, out_ref):
    total = x_ref[0].astype(F32)
    for i in range(1, x_ref.shape[0]):
        total = total + x_ref[i].astype(F32)
    last = total[:, WIDE - 128 :]
    scale = lax.rsqrt((last[:, 112:113] + last[:, 113:114]) / D + EPSILON)

    def act(gate, up):
        gate, up = scale * gate, scale * up
        return (gate * jax.nn.sigmoid(gate) * up).astype(BF)

    head = act(total[:, :HEAD], total[:, HEAD : 2 * HEAD])
    tail = act(last, pltpu.roll(last, 64, 1))[:, :TAIL]
    for i in range(out_ref.shape[0]):
        out_ref[i, :, :HEAD] = head
        out_ref[i, :, HEAD:] = tail


def out_kernel(spans):
    def kernel(x_ref, *refs):
        out_ref = refs[-1]
        groups, rows, width = x_ref.shape
        x = x_ref[...].reshape(groups * rows, width)
        for core in range(2):
            columns = []
            for chip in range(2):
                blocks = [
                    refs[2 * source + chip][core, start : start + count]
                    for source, start, count in spans
                ]
                columns.append(blocks[0] if len(blocks) == 1 else jnp.concatenate(blocks, axis=0))
            part = dot(x, jnp.concatenate(columns, axis=1)).astype(BF)
            out_ref[:, 256 * core : 256 * (core + 1)] = part

    return kernel


def residual_kernel(factor):
    def kernel(at_ref, sum_ref, old_ref, new_ref, copies_ref):
        total = sum_ref[0].astype(F32)
        for i in range(1, sum_ref.shape[0]):
            total = total + sum_ref[i].astype(F32)
        new = (old_ref[at_ref[0]].astype(F32) + factor * total).astype(BF)
        new_ref[0] = new
        for i in range(copies_ref.shape[0]):
            copies_ref[i] = new

    return kernel


def last_kernel(at_ref, sum_ref, old_ref, out_ref):
    total = sum_ref[0].astype(F32)
    for i in range(1, sum_ref.shape[0]):
        total = total + sum_ref[i].astype(F32)
    new = (old_ref[0].astype(F32) + 0.5 * total).astype(BF)
    first = at_ref[0] == 0
    for core in range(2):
        own = new[:, 256 * core : 256 * core + 128]
        other = new[:, 256 * core + 128 : 256 * (core + 1)]
        blocks = (jnp.where(first, own, other), jnp.where(first, other, own))
        for pair in range(2):
            for i in range(16):
                out_ref[(2 * pair + core) * 16 + i] = blocks[pair]


def unpack_kernel(upper_ref, came_ref, out_ref):
    for group in range(8):
        for role in range(2):
            base = role if group < 4 else 1 - role
            chip = upper_ref[0] if base == 0 else 1 - upper_ref[0]
            for core in range(2):
                out_ref[group, role, core] = came_ref[chip, core, group]


def call(kernel, out_shapes, scalars=0):
    smem = pl.BlockSpec(memory_space=pltpu.SMEM)
    vmem = pl.BlockSpec(memory_space=pltpu.VMEM)

    def run(*args):
        return pl.pallas_call(
            kernel,
            in_specs=[smem] * scalars + [vmem] * (len(args) - scalars),
            out_specs=jax.tree.map(lambda s: vmem, out_shapes),
            out_shape=out_shapes,
            compiler_params=pltpu.CompilerParams(vmem_limit_bytes=12 * 2**20),
        )(*args)

    return run


def half_step(wide, down):
    came = exchange(wide.reshape(8, 16, WIDE), "zq")
    hidden = call(act_kernel, jax.ShapeDtypeStruct((8, 16, FFL), BF))(came)
    hidden = exchange(hidden, "zq")
    spans, weights = down
    part = call(out_kernel(spans), jax.ShapeDtypeStruct((128, 512), BF))(hidden, *weights)
    return exchange(part.reshape(16, 8, 512), "tp")


def cell_kernel(at_ref, bias_ref, x_ref, memory_ref, normalizer_ref, stabilizer_ref, *out_refs):
    copies_ref, carried_ref, value_ref, key_ref, normalizer_out, stabilizer_out = out_refs
    total = x_ref[0].astype(F32)
    for i in range(1, x_ref.shape[0]):
        total = total + x_ref[i].astype(F32)
    gates = total[:, 512:]
    scale = lax.rsqrt((gates[:, 112:113] + gates[:, 113:114]) / D + EPSILON)
    query, key, value, outgate = (
        (scale * total[:, 128 * i : 128 * (i + 1)]).astype(BF).astype(F32) for i in range(4)
    )
    key = key * 128 ** (-0.5)
    column = lax.broadcasted_iota(jnp.int32, gates.shape, 1)

    def own_head(at):
        return jnp.sum(jnp.where(column == at, gates, 0.0), axis=1, keepdims=True)

    ingate = scale * own_head(at_ref[0])
    forget = scale * own_head(16 + at_ref[0]) + bias_ref[0]
    log_forget = -(jnp.maximum(-forget, 0.0) + jnp.log1p(jnp.exp(-jnp.abs(forget))))
    diagonal = lax.broadcasted_iota(jnp.int32, (16, 16), 0) == lax.broadcasted_iota(
        jnp.int32, (16, 16), 1
    )
    stabilizer = jnp.sum(jnp.where(diagonal, stabilizer_ref[...], 0.0), axis=1, keepdims=True)
    ceiling = jnp.maximum(log_forget + stabilizer, ingate)
    fresh = jnp.exp(ingate - ceiling)
    carried = jnp.exp(log_forget + stabilizer - ceiling)
    own = jnp.sum(query * key, axis=1, keepdims=True) * fresh
    recall = [
        jnp.sum(memory_ref[i] * query[i : i + 1], axis=1, keepdims=True) for i in range(16)
    ]
    recall = jnp.concatenate(recall + [jnp.zeros((128, 112), F32)], axis=1).T[:16]
    normalizer = normalizer_ref[...]
    denominator = own + carried * jnp.sum(normalizer * query, axis=1, keepdims=True)
    numerator = own * value + carried * recall
    readout = numerator / jnp.maximum(jnp.abs(denominator), jnp.exp(-ceiling))
    gated = (jax.nn.sigmoid(outgate) * readout).astype(BF)
    for i in range(copies_ref.shape[0]):
        copies_ref[i] = gated
    carried_ref[...] = jnp.broadcast_to(carried, carried_ref.shape)
    value_ref[...] = fresh * value
    key_ref[...] = key
    normalizer_out[...] = carried * normalizer + fresh * key
    stabilizer_out[...] = jnp.sum(jnp.where(diagonal, ceiling, 0.0), axis=0, keepdims=True)


def on_device(
    tokens,
    gain_first,
    gate_first,
    up_first,
    down_first,
    gain_mix,
    w_query,
    w_key,
    w_value,
    w_outgate,
    w_ingate,
    w_forget,
    forget_bias,
    memory,
    normalizer,
    stabilizer,
    w_project,
    gain_second,
    gate_second,
    up_second,
    down_second,
):
    pair = lax.axis_index("zp")
    core = lax.axis_index("c")
    at = lax.axis_index("tp")

    pair_at = jnp.reshape(pair, (1,)).astype(jnp.int32)
    upper = (lax.axis_index("zq") >= 4).astype(jnp.int32)
    upper_at = jnp.reshape(upper, (1,))
    role_at = pair_at + upper_at - 2 * pair_at * upper_at
    core_at = jnp.reshape(core, (1,)).astype(jnp.int32)
    shard_at = jnp.reshape(at, (1,)).astype(jnp.int32)
    zero = jnp.zeros((1,), jnp.int32)
    wide_shape = jax.ShapeDtypeStruct((128, WIDE), BF)

    smem = pl.BlockSpec(memory_space=pltpu.SMEM)
    vmem = pl.BlockSpec(memory_space=pltpu.VMEM)
    packed = jax.ShapeDtypeStruct((HERE + WIDE, 128), BF)
    kept, sent = pl.pallas_call(
        prep_kernel,
        in_specs=[smem] + [vmem] * 4 + [pl.BlockSpec(memory_space=pl.ANY)] * 2,
        out_specs=(vmem, vmem),
        out_shape=(packed, packed),
        scratch_shapes=[pltpu.SemaphoreType.DMA((12,))],
        name="prep",
        compiler_params=pltpu.CompilerParams(vmem_limit_bytes=4 * 2**20),
    )(
        role_at,
        tokens.reshape(8, NP, 2, 16, 128),
        gain_first.reshape(1, 128),
        gain_mix.reshape(1, 128),
        gain_second.reshape(1, 128),
        gate_first.T,
        up_first.T,
    )
    came = swap(sent)
    heads = w_ingate.shape[1]
    middle = pack(
        [(i, 0, 128) for i in range(4)]
        + [(4, 0, heads), (5, 0, heads), (6, 0, 128), (7, FFL - 64, 64), (8, 0, FFL)],
        w_query,
        w_key,
        w_value,
        w_outgate,
        w_ingate.T,
        w_forget.T,
        w_project,
        down_second,
        down_first,
    )
    middle_came = swap(middle)
    last = pack(gate_up(0, 1) + [(2, 0, FFL - 64)], gate_second.T, up_second.T, down_second)
    last_came = swap(last)

    first_own, first_other = both_cores(kept), both_cores(came)
    middle_own, middle_other = both_cores(middle[:736]), both_cores(middle_came[:736])
    down_own, down_other = both_cores(down_first), both_cores(middle_came[736:])
    last_own = both_cores(last)
    last_other = both_cores(last_came)

    shard = jax.ShapeDtypeStruct((1, 8, 512), BF)
    copied = jax.ShapeDtypeStruct((16, 8, 512), BF)
    wide, rows, gains = call(
        first_kernel, (wide_shape, copied, jax.ShapeDtypeStruct((3, 1, 512), F32)), 1
    )(core_at, first_own, first_other)
    came = half_step(wide, (((0, 0, FFL),), (down_own, down_other)))
    after_first, copies = call(residual_kernel(0.5), (shard, copied), 1)(shard_at, came, rows)
    copies = exchange(copies, "tp")

    mixed = call(mix_kernel, jax.ShapeDtypeStruct((128, MIX), BF))(
        copies, gains, middle_own, middle_other
    )
    summed = exchange(mixed.reshape(8, 16, MIX), "zq")
    small = jax.ShapeDtypeStruct((16, 128), F32)
    copies, carried, value, key, normalizer_new, stabilizer_new = call(
        cell_kernel,
        (jax.ShapeDtypeStruct((8, 16, 128), BF), small, small, small, small, jax.ShapeDtypeStruct((1, 16), F32)),
        2,
    )(
        shard_at,
        forget_bias,
        summed,
        memory.reshape(16, 128, 128),
        normalizer.reshape(16, 128),
        stabilizer.T,
    )
    memory_new = (
        carried[:, None, :1, None] * memory + value[:, None, :, None] * key[:, None, None, :]
    )
    normalizer_new = normalizer_new.reshape(normalizer.shape)
    stabilizer_new = stabilizer_new.T
    gated = exchange(copies, "zq")
    part = call(out_kernel(((0, 544, 128),)), jax.ShapeDtypeStruct((128, 512), BF))(
        gated, middle_own, middle_other
    )
    came = exchange(part.reshape(16, 8, 512), "tp")
    after_mix, copies = call(residual_kernel(1.0), (shard, copied), 1)(zero, came, after_first)
    copies = exchange(copies, "tp")

    wide = call(wide_kernel, wide_shape)(copies, gains, last_own, last_other)
    came = half_step(
        wide,
        (
            ((0, WIDE, FFL - 64), (1, 672, 64)),
            (last_own, last_other, middle_own, middle_other),
        ),
    )
    outgoing = call(last_kernel, jax.ShapeDtypeStruct((64, 8, 128), BF), 1)(
        pair_at, came, after_mix
    )
    came = exchange(outgoing, ("zp", "c", "tp"))
    out = call(unpack_kernel, jax.ShapeDtypeStruct((8, NP, 2, 16, 128), BF), 1)(
        upper_at, came.reshape(NP, 2, 8, 16, 128)
    )
    return (out.reshape(-1, 128), memory_new, normalizer_new, stabilizer_new)


def solution(mesh):
    kv, tp = mesh.shape["kv"], mesh.shape["tp"]
    finer = Mesh(mesh.devices.reshape(kv // (2 * NP), NP, 2, tp), ("zq", "zp", "c", "tp"))
    return jax.shard_map(
        on_device,
        mesh=finer,
        in_specs=(
            P(None, KV),
            P(KV),
            P(KV, "tp"),
            P(KV, "tp"),
            P("tp", KV),
            P(KV),
            P(KV, "tp"),
            P(KV, "tp"),
            P(KV, "tp"),
            P(KV, "tp"),
            P(KV, None),
            P(KV, None),
            P("tp"),
            P(KV, "tp", None, None),
            P(KV, "tp", None),
            P(KV, "tp"),
            P("tp", KV),
            P(KV),
            P(KV, "tp"),
            P(KV, "tp"),
            P("tp", KV),
        ),
        out_specs=(P(None, KV), P(KV, "tp", None, None), P(KV, "tp", None), P(KV, "tp")),
        check_vma=False,
    )
```
